1024 devices in a mesh: sp: 256 (over z, x, core), tp: 4 (over y).
Axes of the slice: x: 4, y: 4, z: 32, core: 2. Of those that a mesh axis runs over, the one named last changes fastest.
Arguments:
- proj_value: bfloat16 [98304, 1024], P('sp', 'tp'), may hold values from -6 to 6
- proj_gate: bfloat16 [98304, 1024], P('sp', 'tp'), may hold values from -8 to 8
- out_cotangent: bfloat16 [98304, 2048], P('sp'), may hold values from -24 to 24
- out_weight: bfloat16 [1024, 2048], P('tp'), may hold values from -0.1875 to 0.1875
- conv_taps: bfloat16 [31, 1024], P(None, 'tp'), may hold values from -1 to 1
- norm_gain: float32 [1024], P('tp'), may hold values from 0.1 to 1.9
- row_mean: float32 [98304], P('sp'), may hold values from -2 to 2
- row_scale: float32 [98304], P('sp'), may hold values from 0.7 to 3
Outputs:
- value_grad: bfloat16 [98304, 1024], P('sp', 'tp')
- gate_grad: bfloat16 [98304, 1024], P('sp', 'tp')
- out_weight_grad: float32 [2048, 1024], P('sp', 'tp')
- taps_grad: float32 [31, 1024], P(None, 'tp')
- gain_grad: float32 [1024], P('tp')
The draws below stay inside these ranges and needn't reach their ends.
All inputs are finite; a program needn't handle non-finite values.
Results may differ from the reference program's by a relative error of at most 0.0047.
Values may be sent and summed in bfloat16 or wider, within the bound.
A program may use at most 32 MiB of HBM per device.

```python
import math
import jax
import jax.numpy as jnp

D = 2048
CH = 1024
CONV_K = 31
TOKENS = 98304


def with_spikes(values, key, source, target, shards_of, factor):
    owner, partner = [(jnp.arange(values.shape[dim]) // (values.shape[dim] // shards_of)).reshape([-1 if axis == dim else 1 for axis in range(values.ndim)]) for dim in (source, target)]
    chosen = jax.random.permutation(key, shards_of)[partner]
    strong = (owner == chosen) | (owner == (partner + shards_of // 2) % shards_of)
    return jnp.where(strong, factor * values, values)


def level_of(rng, shape, pieces, least, top_value):
    def one(position, blocks):
        steps = jax.random.uniform(jax.random.fold_in(jax.random.fold_in(rng, 6), position), (blocks,), jnp.float32, least / len(pieces), top_value / len(pieces))
        return jnp.repeat(jnp.exp(steps), shape[position] // blocks).reshape((-1,) + (1,) * (len(shape) - position - 1))

    factor_of = one(*pieces[0])
    for cut in pieces[1:]:
        factor_of = factor_of * one(*cut)
    return factor_of


def noise(own_key, shape, scale, most, split=(), held_as=jnp.bfloat16):
    factor_of = level_of(own_key, shape, split, -0.22, 0.18) if split else 1.0
    result = jax.random.normal(own_key, shape, jnp.float32) * scale * factor_of
    return jnp.minimum(jnp.maximum(result, -most), most).astype(held_as)


def bell_draw_with(stream_key, extent, width, reach, shards, heavy, held_as=jnp.bfloat16):
    result = width * jax.random.normal(stream_key, extent, jnp.float32)
    if shards:
        result = result * level_of(stream_key, extent, shards, -0.22, 0.18)
    return jnp.clip(with_spikes(result, jax.random.fold_in(stream_key, 3), *heavy), -reach, reach).astype(held_as)


def setup_inputs(seed: int = 0) -> dict:
    key_list = jax.random.split(jax.random.key(seed), 9)
    proj_value = noise(key_list[0], (TOKENS, CH), 1.0, 6.0, ((0, 256), (1, 4)))
    proj_gate = noise(key_list[1], (TOKENS, CH), 1.5, 8.0, ((0, 256), (1, 4)))
    out_cotangent = bell_draw_with(key_list[2], (TOKENS, D), 1.0, 24.0, ((0, 256),), (0, 1, 256, 6.0))
    out_weight = noise(key_list[3], (CH, D), CH ** -0.5, 0.1875, ((0, 4),))
    conv_taps = noise(key_list[4], (CONV_K, CH), CONV_K ** -0.5, 1.0, ((1, 4),))
    norm_gain = jnp.clip(1.0 + 0.18 * jax.random.normal(key_list[5], (CH,), jnp.float32), 0.1, 1.9)
    row_mean = noise(key_list[6], (TOKENS,), 0.3, 2.0, ((0, 256),), jnp.float32)
    row_scale = jnp.clip(jnp.exp(math.log(3.0) - 1.4552872 * jax.random.uniform(key_list[7], (TOKENS,), jnp.float32) ** level_of(key_list[7], (TOKENS,), ((0, 256),), -0.2, 0.2)), 0.7, 3.0)
    return {"proj_value": proj_value, "proj_gate": proj_gate, "out_cotangent": out_cotangent, "out_weight": out_weight, "conv_taps": conv_taps, "norm_gain": norm_gain, "row_mean": row_mean, "row_scale": row_scale}


def reference(proj_value, proj_gate, out_cotangent, out_weight, conv_taps, norm_gain, row_mean, row_scale):
    kernel = conv_taps.shape[0]
    length = proj_value.shape[0]
    channels = proj_value.shape[1]
    gate_sig = jax.nn.sigmoid(proj_gate.astype(jnp.float32))
    gated = (proj_value.astype(jnp.float32) * gate_sig).astype(jnp.bfloat16)
    padded = jnp.concatenate([jnp.zeros((kernel - 1, channels), jnp.bfloat16), gated], 0).astype(jnp.float32)
    taps_wide = conv_taps.astype(jnp.float32)
    conv = jnp.zeros((length, channels), jnp.float32)
    for offset in range(kernel):
        conv = conv + taps_wide[offset][None, :] * padded[offset:offset + length]
    normed = (conv - row_mean[:, None]) * row_scale[:, None]
    gain_wide = norm_gain.astype(jnp.float32)
    active = normed * gain_wide[None, :]
    sig_act = jax.nn.sigmoid(active)
    hidden = (active * sig_act).astype(jnp.bfloat16)
    upstream = jnp.dot(out_cotangent, out_weight.T, preferred_element_type=jnp.float32)
    weight_grad = jnp.dot(out_cotangent.T, hidden, preferred_element_type=jnp.float32)
    d_active = upstream * sig_act * (1.0 + active * (1.0 - sig_act))
    gain_grad = jnp.sum(d_active * normed, 0)
    d_normed = d_active * gain_wide[None, :]
    first = jnp.mean(d_normed, 1)
    second = jnp.mean(d_normed * normed, 1)
    d_conv = row_scale[:, None] * (d_normed - first[:, None] - normed * second[:, None])
    taps_grad = jnp.stack([jnp.sum(d_conv * padded[offset:offset + length], 0) for offset in range(kernel)])
    extended = jnp.concatenate([d_conv, jnp.zeros((kernel - 1, channels), jnp.float32)], 0)
    d_gated = jnp.zeros((length, channels), jnp.float32)
    for offset in range(kernel):
        begin = kernel - 1 - offset
        d_gated = d_gated + taps_wide[offset][None, :] * extended[begin:begin + length]
    value_grad = (d_gated * gate_sig).astype(jnp.bfloat16)
    gate_grad = (d_gated * proj_value.astype(jnp.float32) * gate_sig * (1.0 - gate_sig)).astype(jnp.bfloat16)
    return value_grad, gate_grad, weight_grad, taps_grad, gain_grad
```

```python
import functools

import jax
import jax.numpy as jnp
from jax import lax
from jax.experimental import pallas as pl
from jax.experimental.pallas import tpu as pltpu
from jax.sharding import Mesh
from jax.sharding import PartitionSpec as P

MESH = pl.DeviceIdType.MESH
SP = ("z", "x", "c")
NZ, NX, NC, NY = 32, 4, 2, 4
F32, BF16 = jnp.float32, jnp.bfloat16
HALO = 32
NEAR = 4
CHUNKS = 4


def sigmoid(v):
    return 1.0 / (1.0 + jnp.exp(-v))


def main_kernel(
    pv_h, pg_h, cot_h, ow_h, taps_h, gain_h, mean_h, scale_h,
    vg_o, gg_o, wg_o, tg_o, gn_o,
    pv, pg, cot, ow, taps_b, gain_v, mean_v, scale_v,
    hs, hr, gp, sg, us, cv, nm, dn, hid, dcp, rm, rs, s1, s2, wt, gacc,
    ys, yr, tacc, tp, tr, tz, tf, w32, wc, wo, xs, xr, zs, zo, zr,
    in_sem, halo_sem, dhalo_sem, y_ss, y_rs, t_ss, t_rs, tz_ss, tz_rs, tf_ss, tf_rs,
    c_ss, c_rs, x_ss, x_rs, z_ss, z_rs, far_sem,
):
    length = pv.shape[0]
    taps = taps_b.shape[0]
    z, x, c, y = (lax.axis_index(a) for a in ("z", "x", "c", "y"))
    j_me = x * NC + c
    rem, div = lax.rem, lax.div

    def copy_in(src, dst, k):
        cp = pltpu.make_async_copy(src, dst, in_sem.at[k])
        cp.start()
        return cp

    in_pv = copy_in(pv_h, pv, 0)
    in_pg = copy_in(pg_h, pg, 1)
    in_small = [copy_in(s, d, 2 + k) for k, (s, d) in enumerate(
        ((taps_h, taps_b), (gain_h, gain_v), (mean_h, mean_v), (scale_h, scale_v)))]
    in_ow = copy_in(ow_h, ow, 6)
    part = length // 3
    in_cot = [copy_in(cot_h.at[pl.ds(part * k, part), :], cot.at[pl.ds(part * k, part), :], 7 + k) for k in range(3)]

    plane = []
    for q in range(1, NX * NC):
        plane.append((rem(x + q // NC, NX), rem(c + q % NC, NC)))
    xs_of = [rem(x + q, NX) for q in range(1, NX)]
    nxt = {"z": rem(z + div(x + c, NX), NZ), "x": rem(x + c, NX), "c": 1 - c}
    nxt["z"] = rem(z + div(x * NC + c + 1, NX * NC), NZ)
    prv = {"z": rem(z + NZ - 1 + div(x + NX - 1 + c, NX), NZ), "x": rem(x + NX - 1 + c, NX), "c": 1 - c}

    barrier = pltpu.get_barrier_semaphore()
    near = [{"x": px, "c": pc} for px, pc in plane] + [{"y": rem(y + q, NY)} for q in range(1, NY)] + [nxt, prv]
    near += [{"z": rem(z + q, NZ)} for q in range(1, NEAR + 1)] + [{"z": rem(z + NZ - q, NZ)} for q in range(1, NEAR + 1)]
    for to in near:
        pl.semaphore_signal(barrier, inc=1, device_id=to, device_id_type=MESH)

    in_pv.wait()
    in_pg.wait()

    def gate_rows(r0, rows):
        for h in range(2):
            lanes = pl.ds(128 * h, 128)
            s = sigmoid(pg[pl.ds(r0, rows), lanes].astype(F32))
            g = (pv[pl.ds(r0, rows), lanes].astype(F32) * s).astype(BF16)
            sg[h, pl.ds(r0, rows), :] = s
            gp[h, pl.ds(r0 + HALO, rows), :] = g.astype(F32)
            yield lanes, g

    for lanes, g in gate_rows(length - HALO, HALO):
        hs[:, lanes] = g
    pl.semaphore_wait(barrier, len(near))
    halo = pltpu.make_async_remote_copy(hs, hr, halo_sem.at[0], halo_sem.at[1], device_id=nxt, device_id_type=MESH)
    halo.start()

    @pl.loop(0, (length - HALO) // 32)
    def _(i):
        for _ in gate_rows(pl.multiple_of(i * 32, 32), 32):
            pass

    for cp in in_small:
        cp.wait()
    for h in range(2):
        wt[h, 0:taps, :] = taps_b[:, pl.ds(128 * h, 128)].astype(F32)
    gain = [gain_v[pl.ds(128 * h, 128)].reshape(1, 128) for h in range(2)]
    for b in range(length // 128):
        rows = pl.ds(128 * b, 128)
        rm[rows, :] = jnp.broadcast_to(mean_v[rows].reshape(1, 128), (128, 128)).T
        rs[rows, :] = jnp.broadcast_to(scale_v[rows].reshape(1, 128), (128, 128)).T

    in_ow.wait()
    for k, cp in enumerate(in_cot):
        cp.wait()
        rows = pl.ds(part * k, part)
        u = lax.dot_general(cot[rows, :], ow[...], (((1,), (1,)), ((), ())), preferred_element_type=F32)
        for h in range(2):
            us[h, rows, :] = u[:, 128 * h:128 * h + 128]

    def conv_rows(h, r0, rows):
        acc = jnp.zeros((rows, 128), F32)
        for k in range(taps):
            acc = acc + wt[h, k:k + 1, :] * gp[h, pl.ds(r0 + (HALO + 1 - taps + k), rows), :]
        cv[h, pl.ds(r0, rows), :] = acc

    def point_rows(r0, rows):
        sl = pl.ds(r0, rows)
        sums = []
        for h in range(2):
            n = (cv[h, sl, :] - rm[sl, :]) * rs[sl, :]
            a = n * gain[h]
            s = sigmoid(a)
            hid[sl, pl.ds(128 * h, 128)] = (a * s).astype(BF16)
            da = us[h, sl, :] * s * (1.0 + a * (1.0 - s))
            d = da * gain[h]
            dan = da * n
            gacc[h, :, :] += dan.reshape(rows // 8, 8, 128).sum(axis=0)
            nm[h, sl, :] = n
            dn[h, sl, :] = d
            sums.append((d, dan * gain[h]))
        s1[sl, :] = sums[0][0] + sums[1][0]
        s2[sl, :] = sums[0][1] + sums[1][1]

    gacc[...] = jnp.zeros_like(gacc)

    @pl.loop(0, 8)
    def _(i):
        conv_rows(rem(i, 2), pl.multiple_of(HALO + div(i, 2) * 88, 8), 88)

    @pl.loop(0, (length - HALO) // 32)
    def _(i):
        point_rows(pl.multiple_of(HALO + i * 32, 32), 32)

    def row_sums(b):
        rows = pl.ds(128 * b, 128)
        ys[0:1, rows] = jnp.sum(s1[rows, :].T, axis=0, keepdims=True)
        ys[1:2, rows] = jnp.sum(s2[rows, :].T, axis=0, keepdims=True)

    row_sums(1)
    row_sums(2)

    def far(step, k):
        for to in (rem(z + step, NZ), rem(z + NZ - step, NZ)):
            pl.semaphore_signal(far_sem.at[k], inc=1, device_id={"z": to}, device_id_type=MESH)

    far(NEAR, 0)

    halo.wait_recv()
    first_dev = (z * (NX * NC) + j_me) == 0
    for h in range(2):
        got = hr[:, pl.ds(128 * h, 128)].astype(F32)
        gp[h, 0:HALO, :] = jnp.where(first_dev, jnp.zeros_like(got), got)
        conv_rows(h, 0, HALO)
    point_rows(0, HALO)
    row_sums(0)

    y_cp = []
    yr[y] = ys[...]
    for q in range(1, NY):
        y_cp.append(pltpu.make_async_remote_copy(
            ys, yr.at[y], y_ss.at[q], y_rs.at[q], device_id={"y": rem(y + q, NY)}, device_id_type=MESH))
        y_cp[-1].start()

    pl.semaphore_wait(far_sem.at[0], 2)
    far(2 * NEAR, 1)

    zc = NZ // CHUNKS
    c_cp = []
    for k in range(CHUNKS):
        @pl.loop(0, zc // 2)
        def _(i):
            lanes = pl.ds(pl.multiple_of((k * (zc // 2) + i) * 128, 128), 128)
            w = lax.dot_general(cot[:, lanes], hid[...], (((0,), (0,)), ((), ())), preferred_element_type=F32)
            for e in range(2):
                for px in range(NX):
                    for pc in range(NC):
                        r = 64 * e + 16 * px + 8 * pc
                        for h in range(2):
                            w32[k, pc, px, 2 * i + e, h, :, :] = w[r:r + 8, 128 * h:128 * h + 128]
        c_cp.append(pltpu.make_async_remote_copy(
            w32.at[k, 1 - c], wc.at[k], c_ss.at[k], c_rs.at[k], device_id={"c": 1 - c}, device_id_type=MESH))
        c_cp[-1].start()

    x_cp = []

    def x_phase(k):
        c_cp[k].wait_recv()

        @pl.loop(0, NX * zc)
        def _(i):
            px, e = div(i, zc), rem(i, zc)
            v = (w32[k, c, px, e] + wc[k, px, e]).reshape(16, 128)
            xs[k, px, e] = v.astype(BF16)

            @pl.when(px == x)
            def _():
                wo[k * zc + e] = v
        for q in (2, 1, 3):
            to = rem(x + q, NX)
            x_cp.append(pltpu.make_async_remote_copy(
                xs.at[k, to], xr.at[q - 1, k], x_ss.at[q, k], x_rs.at[q, k], device_id={"x": to}, device_id_type=MESH))
            x_cp[-1].start()

    x_phase(0)
    x_phase(1)

    for cp in y_cp:
        cp.wait_recv()
    inv = 1.0 / (NY * pv.shape[1])
    tot = ((yr[0] + yr[1]) + (yr[2] + yr[3])) * inv
    for b in range(length // 128):
        rows = pl.ds(128 * b, 128)
        s1[rows, :] = jnp.broadcast_to(tot[0:1, 128 * b:128 * b + 128], (128, 128)).T
        s2[rows, :] = jnp.broadcast_to(tot[1:2, 128 * b:128 * b + 128], (128, 128)).T

    @pl.loop(0, length // 32)
    def _(i):
        sl = pl.ds(pl.multiple_of(i * 32, 32), 32)
        for h in range(2):
            dcp[h, sl, :] = rs[sl, :] * (dn[h, sl, :] - s1[sl, :] - nm[h, sl, :] * s2[sl, :])

    dhalo = pltpu.make_async_remote_copy(
        dcp.at[:, pl.ds(0, HALO), :], dcp.at[:, pl.ds(length, HALO), :], dhalo_sem.at[0], dhalo_sem.at[1],
        device_id=prv, device_id_type=MESH)
    dhalo.start()

    for h in range(2):
        def tap_rows(i, acc):
            r0 = pl.multiple_of(i * 8, 8)
            d = dcp[h, pl.ds(r0, 8), :]
            return tuple(acc[k] + d * gp[h, pl.ds(r0 + (HALO + 1 - taps + k), 8), :] for k in range(taps))
        acc = lax.fori_loop(0, length // 8, tap_rows, tuple(jnp.zeros((8, 128), F32) for _ in range(taps)))
        for k in range(taps):
            tp[k // 4, 4 * h + k % 4, :] = jnp.sum(acc[k], axis=0)
        tp[taps // 4, 4 * h + taps % 4, :] = jnp.sum(gacc[h], axis=0)

    t_cp = []
    tr[j_me] = tp[j_me]
    for q, (px, pc) in enumerate(plane):
        t_cp.append(pltpu.make_async_remote_copy(
            tp.at[px * NC + pc], tr.at[j_me], t_ss.at[q], t_rs.at[q], device_id={"x": px, "c": pc}, device_id_type=MESH))
        t_cp[-1].start()

    pl.semaphore_wait(far_sem.at[1], 2)
    x_phase(2)
    x_phase(3)

    for cp in t_cp:
        cp.wait_recv()
    share = tr[0]
    for j in range(1, NX * NC):
        share = share + tr[j]
    tz[z] = share
    tf[0] = share

    def z_copy(src, dst, ss, rs_, d):
        return pltpu.make_async_remote_copy(
            src, dst, ss.at[d], rs_.at[d], device_id={"z": rem(z + d, NZ)}, device_id_type=MESH)

    def by_distance(i):
        half = div(i + 1, 2)
        return NZ // 2 + half * (1 - 2 * rem(i, 2))

    @pl.loop(0, NZ - 1)
    def _(i):
        d = by_distance(i)
        z_copy(tf.at[0], tz.at[z], tz_ss, tz_rs, d).start()

    for cp in x_cp:
        cp.wait_recv()

    @pl.loop(0, NZ)
    def _(i):
        k, e = div(i, zc), rem(i, zc)
        v = wo[i] + (xr[0, k, e].astype(F32) + xr[1, k, e].astype(F32)) + xr[2, k, e].astype(F32)
        zs[i] = v.astype(BF16)

        @pl.when(i == z)
        def _():
            zo[...] = v

    @pl.loop(0, NZ - 1)
    def _(i):
        d = by_distance(i)
        z_copy(zs.at[rem(z + d, NZ)], zr.at[z], z_ss, z_rs, d).start()

    last_dev = (z * (NX * NC) + j_me) == NZ * NX * NC - 1
    dhalo.wait_recv()
    for h in range(2):
        got = dcp[h, pl.ds(length, HALO), :]
        dcp[h, pl.ds(length, HALO), :] = jnp.where(last_dev, jnp.zeros_like(got), got)

    for h in range(2):
        @pl.loop(0, length // 64)
        def _(i):
            r0 = pl.multiple_of(i * 64, 64)
            acc = jnp.zeros((64, 128), F32)
            for k in range(taps):
                acc = acc + wt[h, k:k + 1, :] * dcp[h, pl.ds(r0 + (taps - 1 - k), 64), :]
            sl, lanes = pl.ds(r0, 64), pl.ds(128 * h, 128)
            s = sg[h, sl, :]
            vg_o[sl, lanes] = (acc * s).astype(BF16)
            gg_o[sl, lanes] = (acc * pv[sl, lanes].astype(F32) * s * (1.0 - s)).astype(BF16)

    @pl.loop(1, NZ)
    def _(d):
        z_copy(tf.at[0], tz.at[z], tz_ss, tz_rs, d).wait_recv()

    total = lax.fori_loop(1, NZ, lambda i, a: a + tz[i], tz[0])
    tr[j_me] = total
    f_cp = []
    for q, (px, pc) in enumerate(plane):
        f_cp.append(pltpu.make_async_remote_copy(
            tr.at[j_me], tacc.at[j_me], tf_ss.at[q], tf_rs.at[q], device_id={"x": px, "c": pc}, device_id_type=MESH))
        f_cp[-1].start()
    tacc[j_me] = total

    @pl.loop(1, NZ)
    def _(d):
        z_copy(zs.at[0], zr.at[z], z_ss, z_rs, d).wait_recv()
    zr[z] = jnp.zeros((16, 128), BF16)
    wsum = lax.fori_loop(0, NZ, lambda i, a: a + zr[i].astype(F32), zo[...])
    for h in range(2):
        wg_o[:, pl.ds(128 * h, 128)] = wsum[8 * h:8 * h + 8, :]

    for cp in f_cp:
        cp.wait_recv()
    for j in range(NX * NC):
        t = tacc[j]
        for h in range(2):
            for i in range(4):
                row = t[4 * h + i:4 * h + i + 1, :]
                if 4 * j + i < taps:
                    tg_o[4 * j + i:4 * j + i + 1, pl.ds(128 * h, 128)] = row
                else:
                    gn_o[pl.ds(128 * h, 128)] = row.reshape(128)

    halo.wait_send()
    dhalo.wait_send()
    for cp in y_cp + c_cp + x_cp + t_cp + f_cp:
        cp.wait_send()

    @pl.loop(1, NZ)
    def _(d):
        z_copy(tf.at[0], tz.at[z], tz_ss, tz_rs, d).wait_send()
        z_copy(zs.at[0], zr.at[z], z_ss, z_rs, d).wait_send()


def shards(pv, pg, cot, ow, taps, gain, mean, scale):
    length, ch = pv.shape
    d = cot.shape[1]
    zc = NZ // CHUNKS
    V, D = pltpu.VMEM, pltpu.SemaphoreType.DMA
    any_spec, vmem = pl.BlockSpec(memory_space=pl.ANY), pl.BlockSpec(memory_space=pltpu.VMEM)
    scratch = [
        V((length, ch), BF16), V((length, ch), BF16), V((length, d), BF16), V((ch, d), BF16),
        V(taps.shape, BF16), V((ch,), F32), V((length,), F32), V((length,), F32),
        V((HALO, ch), BF16), V((HALO, ch), BF16),
        V((2, length + HALO, 128), F32), V((2, length, 128), F32), V((2, length, 128), F32),
        V((2, length, 128), F32), V((2, length, 128), F32), V((2, length, 128), F32),
        V((length, ch), BF16), V((2, length + HALO, 128), F32),
        V((length, 128), F32), V((length, 128), F32), V((length, 128), F32), V((length, 128), F32),
        V((2, 32, 128), F32), V((2, 8, 128), F32),
        V((2, length), F32), V((NY, 2, length), F32),
        V((8, 8, 128), F32), V((8, 8, 128), F32), V((8, 8, 128), F32), V((NZ, 8, 128), F32), V((1, 8, 128), F32),
        V((CHUNKS, NC, NX, zc, 2, 8, 128), F32), V((CHUNKS, NX, zc, 2, 8, 128), F32),
        V((NZ, 16, 128), F32), V((CHUNKS, NX, zc, 16, 128), BF16), V((NX - 1, CHUNKS, zc, 16, 128), BF16),
        V((NZ, 16, 128), BF16), V((16, 128), F32), V((NZ, 16, 128), BF16),
        D((10,)), D((2,)), D((2,)), D((NY,)), D((NY,)), D((7,)), D((7,)), D((NZ,)), D((NZ,)), D((7,)), D((7,)),
        D((CHUNKS,)), D((CHUNKS,)), D((NX, CHUNKS)), D((NX, CHUNKS)), D((NZ,)), D((NZ,)),
        pltpu.SemaphoreType.REGULAR((2,)),
    ]
    return pl.pallas_call(
        main_kernel,
        out_shape=(
            jax.ShapeDtypeStruct((length, ch), BF16), jax.ShapeDtypeStruct((length, ch), BF16),
            jax.ShapeDtypeStruct((8, ch), F32), jax.ShapeDtypeStruct(taps.shape, F32), jax.ShapeDtypeStruct((ch,), F32),
        ),
        in_specs=[any_spec] * 8,
        out_specs=(vmem,) * 5,
        scratch_shapes=scratch,
        name="conv_back",
        compiler_params=pltpu.CompilerParams(collective_id=0, has_side_effects=True, vmem_limit_bytes=56 * 2**20),
    )(pv, pg, cot, ow, taps, gain, mean, scale)


def solution(mesh):
    split = Mesh(mesh.devices.reshape(NZ, NX, NC, mesh.shape["tp"]), ("z", "x", "c", "y"))
    placed = (P(SP, "y"), P(SP, "y"), P(SP, None), P("y", None), P(None, "y"), P("y"), P(SP), P(SP))
    return jax.shard_map(
        shards, mesh=split, in_specs=placed,
        out_specs=(P(SP, "y"), P(SP, "y"), P(SP, "y"), P(None, "y"), P("y")), check_vma=False,
    )
```

```python
import functools

import jax
import jax.numpy as jnp
from jax import lax
from jax.experimental import pallas as pl
from jax.experimental.pallas import tpu as pltpu
from jax.sharding import Mesh
from jax.sharding import PartitionSpec as P

MESH = pl.DeviceIdType.MESH
SP = ("z", "x", "c")
NZ, NX, NC, NY = 32, 4, 2, 4
F32, BF16 = jnp.float32, jnp.bfloat16
HALO = 32
NEAR = 2
NH = NZ // 2
CHUNKS = 4
HC = NH // CHUNKS


def sigmoid(v):
    return 1.0 / (1.0 + jnp.exp(-v))


def main_kernel(
    pv_h, pg_h, cot_h, ow_h, taps_h, gain_h, mean_h, scale_h,
    vg_o, gg_o, wg_o, tg_o, gn_o,
    pv, pg, cot, ow, taps_b, gain_v, mean_v, scale_v,
    hs, hr, gp, sg, us, cv, nm, dn, hid, dcp, rm, rs, s1, s2, wt, gacc,
    cot_t, ys, yr, kacc, tacc, tp, tr, tz, tf, w32, wc, xs, xr, zs, zo, zr,
    in_sem, halo_sem, dhalo_sem, y_ss, y_rs, t_ss, t_rs, tz_ss, tz_rs, tf_ss, tf_rs,
    c_ss, c_rs, x_ss, x_rs, z_ss, z_rs, far_sem,
):
    length = pv.shape[0]
    taps = taps_b.shape[0]
    blocks = length // 128
    z, x, c, y = (lax.axis_index(a) for a in ("z", "x", "c", "y"))
    rem, div = lax.rem, lax.div
    zh, zp = div(z, 2), rem(z, 2)
    m_me = (zp * NX + x) * NC + c

    def copy_in(src, dst, k):
        cp = pltpu.make_async_copy(src, dst, in_sem.at[k])
        cp.start()
        return cp

    in_pv = copy_in(pv_h, pv, 0)
    in_pg = copy_in(pg_h, pg, 1)
    in_small = [copy_in(s, d, 2 + k) for k, (s, d) in enumerate(
        ((taps_h, taps_b), (gain_h, gain_v), (mean_h, mean_v), (scale_h, scale_v)))]
    in_ow = copy_in(ow_h, ow, 6)
    part = length // 3
    in_cot = [copy_in(cot_h.at[pl.ds(part * k, part), :], cot.at[pl.ds(part * k, part), :], 7 + k) for k in range(3)]

    mates = []
    for dx in (2, 1, 3, 0):
        for dz in range(2):
            for dc in range(NC):
                if dx or dz or dc:
                    mates.append((rem(zp + dz, 2), rem(x + dx, NX), rem(c + dc, NC)))
    wmates = []
    for dx in (2, 1, 3, 0):
        for dz in range(2):
            if dx or dz:
                wmates.append((rem(zp + dz, 2), rem(x + dx, NX), dz * NX + dx - 1))

    def mate(pz, px, pc):
        return {"z": 2 * zh + pz, "x": px, "c": pc}

    nxt = {"z": rem(z + div(x * NC + c + 1, NX * NC), NZ), "x": rem(x + c, NX), "c": 1 - c}
    prv = {"z": rem(z + NZ - 1 + div(x + NX - 1 + c, NX), NZ), "x": rem(x + NX - 1 + c, NX), "c": 1 - c}
    barrier = pltpu.get_barrier_semaphore()
    near = [nxt, prv] + [{"y": rem(y + q, NY)} for q in range(1, NY)]
    near += [{"z": rem(z + NEAR, NZ)}, {"z": rem(z + NZ - NEAR, NZ)}] + [mate(*to) for to in mates]
    for to in near:
        pl.semaphore_signal(barrier, inc=1, device_id=to, device_id_type=MESH)

    in_pv.wait()
    in_pg.wait()

    def gate_rows(r0, rows):
        for h in range(2):
            lanes = pl.ds(128 * h, 128)
            s = sigmoid(pg[pl.ds(r0, rows), lanes].astype(F32))
            g = (pv[pl.ds(r0, rows), lanes].astype(F32) * s).astype(BF16)
            sg[h, pl.ds(r0, rows), :] = s
            gp[h, pl.ds(r0 + HALO, rows), :] = g.astype(F32)
            yield lanes, g
    for lanes, g in gate_rows(length - HALO, HALO):
        hs[:, lanes] = g

    @pl.loop(0, (length - HALO) // 32)
    def _(i):
        for _ in gate_rows(pl.multiple_of(i * 32, 32), 32):
            pass

    for cp in in_small:
        cp.wait()
    for h in range(2):
        wt[h, 0:taps, :] = taps_b[:, pl.ds(128 * h, 128)].astype(F32)
    gain = [gain_v[pl.ds(128 * h, 128)].reshape(1, 128) for h in range(2)]
    for b in range(blocks):
        rows = pl.ds(128 * b, 128)
        rm[rows, :] = jnp.broadcast_to(mean_v[rows].reshape(1, 128), (128, 128)).T
        rs[rows, :] = jnp.broadcast_to(scale_v[rows].reshape(1, 128), (128, 128)).T
    pl.semaphore_wait(barrier, len(near))
    halo = pltpu.make_async_remote_copy(hs, hr, halo_sem.at[0], halo_sem.at[1], device_id=nxt, device_id_type=MESH)
    halo.start()

    def far(step, k):
        for to in (rem(z + step, NZ), rem(z + NZ - step, NZ)):
            pl.semaphore_signal(far_sem.at[k], inc=1, device_id={"z": to}, device_id_type=MESH)

    far(NEAR, 0)

    in_ow.wait()
    for cp in in_cot:
        cp.wait()
    u = lax.dot_general(cot[...], ow[...], (((1,), (1,)), ((), ())), preferred_element_type=F32)
    for h in range(2):
        us[h, :, :] = u[:, 128 * h:128 * h + 128]

    def conv_rows(h, r0, rows):
        acc = jnp.zeros((rows, 128), F32)
        for k in range(taps):
            acc = acc + wt[h, k:k + 1, :] * gp[h, pl.ds(r0 + (HALO + 1 - taps + k), rows), :]
        cv[h, pl.ds(r0, rows), :] = acc

    def point_rows(r0, rows):
        sl = pl.ds(r0, rows)
        sums = []
        for h in range(2):
            n = (cv[h, sl, :] - rm[sl, :]) * rs[sl, :]
            a = n * gain[h]
            s = sigmoid(a)
            hid[sl, pl.ds(128 * h, 128)] = (a * s).astype(BF16)
            da = us[h, sl, :] * s * (1.0 + a * (1.0 - s))
            d = da * gain[h]
            dan = da * n
            gacc[h, :, :] += dan.reshape(rows // 8, 8, 128).sum(axis=0)
            nm[h, sl, :] = n
            dn[h, sl, :] = d
            sums.append((d, dan * gain[h]))
        s1[sl, :] = sums[0][0] + sums[1][0]
        s2[sl, :] = sums[0][1] + sums[1][1]

    gacc[...] = jnp.zeros_like(gacc)
    @pl.loop(0, 8)
    def _(i):
        conv_rows(rem(i, 2), pl.multiple_of(HALO + div(i, 2) * 88, 8), 88)
    pl.semaphore_wait(far_sem.at[0], 2)
    far(2 * NEAR, 1)

    @pl.loop(0, (length - HALO) // 32)
    def _(i):
        point_rows(pl.multiple_of(HALO + i * 32, 32), 32)

    def row_sums(lo, hi):
        for b in range(lo, hi):
            rows = pl.ds(128 * b, 128)
            ys[b, 0:1, :] = jnp.sum(s1[rows, :].T, axis=0, keepdims=True)
            ys[b, 1:2, :] = jnp.sum(s2[rows, :].T, axis=0, keepdims=True)
        cps = []
        for q in (2, 1, 3):
            cps.append(pltpu.make_async_remote_copy(
                ys.at[pl.ds(lo, hi - lo)], yr.at[y, pl.ds(lo, hi - lo)], y_ss.at[q, min(lo, 1)], y_rs.at[q, min(lo, 1)],
                device_id={"y": rem(y + q, NY)}, device_id_type=MESH))
            cps[-1].start()
        return cps
    y_late = row_sums(1, blocks)

    @pl.loop(0, cot.shape[1] // 256)
    def _(i):
        for e in range(2):
            b = pl.multiple_of(i * 256 + 128 * e, 128)
            cot_t[pl.ds(b, 128), :] = cot[:, pl.ds(b, 128)].T
    halo.wait_recv()
    first_dev = ((z * NX + x) * NC + c) == 0
    for h in range(2):
        got = hr[:, pl.ds(128 * h, 128)].astype(F32)
        gp[h, 0:HALO, :] = jnp.where(first_dev, jnp.zeros_like(got), got)
        conv_rows(h, 0, HALO)
    point_rows(0, HALO)
    y_first = row_sums(0, 1)
    yr[y] = ys[...]
    pl.semaphore_wait(far_sem.at[1], 2)
    far(4 * NEAR, 2)

    rows_c = 64 * 2 * HC
    c_cp = []
    for k in range(CHUNKS):
        w = lax.dot_general(
            cot_t[pl.ds(k * rows_c, rows_c), :], hid[...], (((1,), (0,)), ((), ())), preferred_element_type=F32)
        for e in range(HC):
            for pz in range(2):
                for px in range(NX):
                    for pc in range(NC):
                        r = 64 * (2 * e + pz) + 16 * px + 8 * pc
                        for h in range(2):
                            w32[k, pc, pz, px, e, h, :, :] = w[r:r + 8, 128 * h:128 * h + 128]
        c_cp.append(pltpu.make_async_remote_copy(
            w32.at[k, 1 - c], wc.at[k], c_ss.at[k], c_rs.at[k], device_id={"c": 1 - c}, device_id_type=MESH))
        c_cp[-1].start()

    inv = 1.0 / (NY * pv.shape[1])

    def d_conv(lo, hi):
        for b in range(lo, hi):
            rows = pl.ds(128 * b, 128)
            tot = ((yr[0, b] + yr[1, b]) + (yr[2, b] + yr[3, b])) * inv
            s1[rows, :] = jnp.broadcast_to(tot[0:1, :], (128, 128)).T
            s2[rows, :] = jnp.broadcast_to(tot[1:2, :], (128, 128)).T

        @pl.loop(lo * 4, hi * 4)
        def _(i):
            sl = pl.ds(pl.multiple_of(i * 32, 32), 32)
            for h in range(2):
                dcp[h, sl, :] = rs[sl, :] * (dn[h, sl, :] - s1[sl, :] - nm[h, sl, :] * s2[sl, :])

    def tap_rows(lo, hi, start):
        for h in range(2):
            def step(i, acc):
                acc = list(acc)
                for e in range(4):
                    r0 = pl.multiple_of(i * 32 + 8 * e, 8)
                    d = dcp[h, pl.ds(r0, 8), :]
                    for k in range(taps):
                        acc[k] = acc[k] + d * gp[h, pl.ds(r0 + (HALO + 1 - taps + k), 8), :]
                return tuple(acc)
            init = tuple(jnp.zeros((8, 128), F32) if start else kacc[h, k] for k in range(taps))
            acc = lax.fori_loop(lo * 4, hi * 4, step, init)
            for k in range(taps):
                if start:
                    kacc[h, k] = acc[k]
                else:
                    tp[k // 2, 2 * h + k % 2, :] = jnp.sum(acc[k], axis=0)
    for cp in y_late:
        cp.wait_recv()
    d_conv(1, blocks)
    tap_rows(1, blocks, True)
    for h in range(2):
        tp[taps // 2, 2 * h + taps % 2, :] = jnp.sum(gacc[h], axis=0)
    for cp in y_first:
        cp.wait_recv()
    d_conv(0, 1)
    dhalo = pltpu.make_async_remote_copy(
        dcp.at[:, pl.ds(0, HALO), :], dcp.at[:, pl.ds(length, HALO), :], dhalo_sem.at[0], dhalo_sem.at[1],
        device_id=prv, device_id_type=MESH)
    tap_rows(0, 1, False)
    t_cp = []
    for q, to in enumerate(mates):
        t_cp.append(pltpu.make_async_remote_copy(
            tp.at[(to[0] * NX + to[1]) * NC + to[2]], tr.at[m_me], t_ss.at[q], t_rs.at[q],
            device_id=mate(*to), device_id_type=MESH))
        t_cp[-1].start()
    tr[m_me] = tp[m_me]
    dhalo.start()

    x_cp = []
    for k in range(CHUNKS):
        c_cp[k].wait_recv()
        for pz in range(2):
            @pl.loop(0, NX)
            def _(px):
                v = (w32[k, c, pz, px] + wc[k, pz, px]).reshape(HC, 16, 128)
                xs[k, pz, px] = v.astype(BF16)
        for pz, px, q in wmates:
            x_cp.append(pltpu.make_async_remote_copy(
                xs.at[k, pz, px], xr.at[q, k], x_ss.at[q, k], x_rs.at[q, k],
                device_id=mate(pz, px, c), device_id_type=MESH))
            x_cp[-1].start()

    pl.semaphore_wait(far_sem.at[2], 2)
    for cp in t_cp:
        cp.wait_recv()
    share = ((tr[0] + tr[1]) + (tr[2] + tr[3])) + ((tr[4] + tr[5]) + (tr[6] + tr[7]))
    share = share + (((tr[8] + tr[9]) + (tr[10] + tr[11])) + ((tr[12] + tr[13]) + (tr[14] + tr[15])))
    tf[0] = share

    def z_copy(src, dst, ss, rs_, d):
        return pltpu.make_async_remote_copy(
            src, dst, ss.at[d], rs_.at[d], device_id={"z": rem(z + 2 * d, NZ)}, device_id_type=MESH)

    by_distance = [NH // 2]
    for d in range(NH // 2 - 1, 0, -1):
        by_distance += [d, NH - d]
    for d in by_distance:
        z_copy(tf.at[0], tz.at[zh], tz_ss, tz_rs, d).start()
    tz[zh] = share

    for cp in x_cp:
        cp.wait_recv()
    for k in range(CHUNKS):
        v = (w32[k, c, zp, x] + wc[k, zp, x]).reshape(HC, 16, 128)
        for q in range(2 * NX - 1):
            v = v + xr[q, k].astype(F32)
        zo[pl.ds(k * HC, HC)] = v
        zs[pl.ds(k * HC, HC)] = v.astype(BF16)
    for d in by_distance:
        z_copy(zs.at[rem(zh + d, NH)], zr.at[zh], z_ss, z_rs, d).start()

    last_dev = ((z * NX + x) * NC + c) == NZ * NX * NC - 1
    dhalo.wait_recv()
    for h in range(2):
        got = dcp[h, pl.ds(length, HALO), :]
        dcp[h, pl.ds(length, HALO), :] = jnp.where(last_dev, jnp.zeros_like(got), got)
    for h in range(2):
        @pl.loop(0, length // 64)
        def _(i):
            r0 = pl.multiple_of(i * 64, 64)
            acc = jnp.zeros((64, 128), F32)
            for k in range(taps):
                acc = acc + wt[h, k:k + 1, :] * dcp[h, pl.ds(r0 + (taps - 1 - k), 64), :]
            sl, lanes = pl.ds(r0, 64), pl.ds(128 * h, 128)
            s = sg[h, sl, :]
            vg_o[sl, lanes] = (acc * s).astype(BF16)
            gg_o[sl, lanes] = (acc * pv[sl, lanes].astype(F32) * s * (1.0 - s)).astype(BF16)

    for d in range(1, NH):
        z_copy(tf.at[0], tz.at[zh], tz_ss, tz_rs, d).wait_recv()
    parts = [tz[i] for i in range(NH)]
    while len(parts) > 1:
        parts = [a + b for a, b in zip(parts[::2], parts[1::2])]
    total = parts[0]
    tf[1] = total
    f_cp = []
    for q, to in enumerate(mates):
        f_cp.append(pltpu.make_async_remote_copy(
            tf.at[1], tacc.at[m_me], tf_ss.at[q], tf_rs.at[q], device_id=mate(*to), device_id_type=MESH))
        f_cp[-1].start()
    tacc[m_me] = total

    for d in range(1, NH):
        z_copy(zs.at[0], zr.at[zh], z_ss, z_rs, d).wait_recv()
    zr[zh] = jnp.zeros((16, 128), BF16)
    parts = [zo[zh]] + [zr[i].astype(F32) for i in range(NH)]
    while len(parts) > 1:
        parts = [a + b for a, b in zip(parts[::2], parts[1::2])] + parts[len(parts) // 2 * 2:]
    for h in range(2):
        wg_o[:, pl.ds(128 * h, 128)] = parts[0][8 * h:8 * h + 8, :]
    for cp in f_cp:
        cp.wait_recv()
    for k in range(taps + 1):
        for h in range(2):
            row = tacc[k // 2, 2 * h + k % 2:2 * h + k % 2 + 1, :]
            if k < taps:
                tg_o[k:k + 1, pl.ds(128 * h, 128)] = row
            else:
                gn_o[pl.ds(128 * h, 128)] = row.reshape(128)

    halo.wait_send()
    dhalo.wait_send()
    for cp in y_late + y_first + c_cp + x_cp + t_cp + f_cp:
        cp.wait_send()
    for d in range(1, NH):
        z_copy(tf.at[0], tz.at[zh], tz_ss, tz_rs, d).wait_send()
        z_copy(zs.at[0], zr.at[zh], z_ss, z_rs, d).wait_send()


def out_kernel(*refs):
    n = len(refs) // 2
    sems = refs[-1]
    cps = [pltpu.make_async_copy(refs[k], refs[n + k], sems.at[k]) for k in range(n)]
    for cp in cps:
        cp.start()
    for cp in cps:
        cp.wait()


def shards(pv, pg, cot, ow, taps, gain, mean, scale):
    length, ch = pv.shape
    d = cot.shape[1]
    blocks = length // 128
    V, D = pltpu.VMEM, pltpu.SemaphoreType.DMA
    any_spec, vmem = pl.BlockSpec(memory_space=pl.ANY), pl.BlockSpec(memory_space=pltpu.VMEM)
    scratch = [
        V((length, ch), BF16), V((length, ch), BF16), V((length, d), BF16), V((ch, d), BF16),
        V(taps.shape, BF16), V((ch,), F32), V((length,), F32), V((length,), F32),
        V((HALO, ch), BF16), V((HALO, ch), BF16),
        V((2, length + HALO, 128), F32), V((2, length, 128), F32), V((2, length, 128), F32),
        V((2, length, 128), F32), V((2, length, 128), F32), V((2, length, 128), F32),
        V((length, ch), BF16), V((2, length + HALO, 128), F32),
        V((length, 128), F32), V((length, 128), F32), V((length, 128), F32), V((length, 128), F32),
        V((2, 32, 128), F32), V((2, 8, 128), F32),
        V((d, length), BF16),
        V((blocks, 2, 128), F32), V((NY, blocks, 2, 128), F32),
        V((2, 32, 8, 128), F32),
        V((16, 4, 128), F32), V((16, 4, 128), F32), V((16, 4, 128), F32), V((NH, 4, 128), F32), V((2, 4, 128), F32),
        V((CHUNKS, NC, 2, NX, HC, 2, 8, 128), F32), V((CHUNKS, 2, NX, HC, 2, 8, 128), F32),
        V((CHUNKS, 2, NX, HC, 16, 128), BF16), V((2 * NX - 1, CHUNKS, HC, 16, 128), BF16),
        V((NH, 16, 128), BF16), V((NH, 16, 128), F32), V((NH, 16, 128), BF16),
        D((10,)), D((2,)), D((2,)), D((NY, 2)), D((NY, 2)), D((15,)), D((15,)), D((NH,)), D((NH,)), D((15,)), D((15,)),
        D((CHUNKS,)), D((CHUNKS,)), D((2 * NX - 1, CHUNKS)), D((2 * NX - 1, CHUNKS)), D((NH,)), D((NH,)),
        pltpu.SemaphoreType.REGULAR((3,)),
    ]
    outs = (((length, ch), BF16), ((length, ch), BF16), ((8, ch), F32), (taps.shape, F32), ((ch,), F32))
    res = pl.pallas_call(
        main_kernel,
        out_shape=tuple(V(s, t) for s, t in outs),
        in_specs=[any_spec] * 8,
        out_specs=(vmem,) * 5,
        scratch_shapes=scratch,
        name="conv_back",
        compiler_params=pltpu.CompilerParams(collective_id=0, has_side_effects=True, vmem_limit_bytes=56 * 2**20),
    )(pv, pg, cot, ow, taps, gain, mean, scale)
    return pl.pallas_call(
        out_kernel,
        out_shape=tuple(jax.ShapeDtypeStruct(s, t) for s, t in outs),
        in_specs=[vmem] * 5,
        out_specs=(any_spec,) * 5,
        scratch_shapes=[D((5,))],
        name="write_out",
    )(*(pltpu.with_memory_space_constraint(r, pltpu.VMEM) for r in res))


def solution(mesh):
    split = Mesh(mesh.devices.reshape(NZ, NX, NC, mesh.shape["tp"]), ("z", "x", "c", "y"))
    placed = (P(SP, "y"), P(SP, "y"), P(SP, None), P("y", None), P(None, "y"), P("y"), P(SP), P(SP))
    return jax.shard_map(
        shards, mesh=split, in_specs=placed,
        out_specs=(P(SP, "y"), P(SP, "y"), P(SP, "y"), P(None, "y"), P("y")), check_vma=False,
    )
```

```python
import functools

import jax
import jax.numpy as jnp
from jax import lax
from jax.experimental import pallas as pl
from jax.experimental.pallas import tpu as pltpu
from jax.sharding import Mesh
from jax.sharding import PartitionSpec as P

MESH = pl.DeviceIdType.MESH
SP = ("z", "x", "c")
NZ, NX, NC, NY = 32, 4, 2, 4
F32, BF16 = jnp.float32, jnp.bfloat16
HALO = 32
NEAR = 2
NH = NZ // 2
CHUNKS = 4
HC = NH // CHUNKS


def sigmoid(v):
    return 1.0 / (1.0 + jnp.exp(-v))


def main_kernel(
    pv_h, pg_h, cot_h, ow_h, taps_h, gain_h, mean_h, scale_h,
    vg_o, gg_o, wg_o, tg_o, gn_o,
    pv, pg, cot, ow, taps_b, gain_v, mean_v, scale_v,
    hs, hr, gp, sg, us, cv, nm, dn, hid, dcp, rm, rs, s1, s2, wt, gacc,
    cot_t, ys, yr, kacc, tacc, tp, tr, tz, tf, w32, wc, xs, xr, zs, zo, zr,
    in_sem, halo_sem, dhalo_sem, y_ss, y_rs, t_ss, t_rs, tz_ss, tz_rs, tf_ss, tf_rs,
    c_ss, c_rs, x_ss, x_rs, z_ss, z_rs, far_sem,
):
    length = pv.shape[0]
    taps = taps_b.shape[0]
    blocks = length // 128
    z, x, c, y = (lax.axis_index(a) for a in ("z", "x", "c", "y"))
    rem, div = lax.rem, lax.div
    zh, zp = div(z, 2), rem(z, 2)
    g_me = zp * NX + x

    def copy_in(src, dst, k):
        cp = pltpu.make_async_copy(src, dst, in_sem.at[k])
        cp.start()
        return cp

    in_pv = copy_in(pv_h, pv, 0)
    in_pg = copy_in(pg_h, pg, 1)
    in_small = [copy_in(s, d, 2 + k) for k, (s, d) in enumerate(
        ((taps_h, taps_b), (gain_h, gain_v), (mean_h, mean_v), (scale_h, scale_v)))]
    in_ow = copy_in(ow_h, ow, 6)
    part = length // 3
    in_cot = [copy_in(cot_h.at[pl.ds(part * k, part), :], cot.at[pl.ds(part * k, part), :], 7 + k) for k in range(3)]

    steps = [(dx, dz, dc) for dx in (2, 1, 3, 0) for dz in range(2) for dc in range(NC) if dx or dz or dc]
    mates = [(rem(zp + dz, 2), rem(x + dx, NX), rem(c + dc, NC)) for dx, dz, dc in steps]
    owners = []
    for dx in (2, 1, 3, 0):
        for dz in (1, 0):
            owners.append((rem(zp + dz, 2), rem(x + dx, NX), dz * NX + dx))
    wmates = []
    for dx in (2, 1, 3, 0):
        for dz in range(2):
            if dx or dz:
                wmates.append((rem(zp + dz, 2), rem(x + dx, NX), dz * NX + dx - 1))

    def mate(pz, px, pc):
        return {"z": 2 * zh + pz, "x": px, "c": pc}

    nxt = {"z": rem(z + div(x * NC + c + 1, NX * NC), NZ), "x": rem(x + c, NX), "c": 1 - c}
    prv = {"z": rem(z + NZ - 1 + div(x + NX - 1 + c, NX), NZ), "x": rem(x + NX - 1 + c, NX), "c": 1 - c}
    barrier = pltpu.get_barrier_semaphore()
    near = [nxt, prv] + [{"y": rem(y + q, NY)} for q in range(1, NY)]
    near += [{"z": rem(z + NEAR, NZ)}, {"z": rem(z + NZ - NEAR, NZ)}] + [mate(*to) for to in mates]
    for to in near:
        pl.semaphore_signal(barrier, inc=1, device_id=to, device_id_type=MESH)

    in_pv.wait()
    in_pg.wait()

    def gate_rows(r0, rows):
        for h in range(2):
            lanes = pl.ds(128 * h, 128)
            s = sigmoid(pg[pl.ds(r0, rows), lanes].astype(F32))
            g = (pv[pl.ds(r0, rows), lanes].astype(F32) * s).astype(BF16)
            sg[h, pl.ds(r0, rows), :] = s
            gp[h, pl.ds(r0 + HALO, rows), :] = g.astype(F32)
            yield lanes, g
    for lanes, g in gate_rows(length - HALO, HALO):
        hs[:, lanes] = g

    @pl.loop(0, (length - HALO) // 32)
    def _(i):
        for _ in gate_rows(pl.multiple_of(i * 32, 32), 32):
            pass

    for cp in in_small:
        cp.wait()
    for h in range(2):
        wt[h, 0:taps, :] = taps_b[:, pl.ds(128 * h, 128)].astype(F32)
    gain = [gain_v[pl.ds(128 * h, 128)].reshape(1, 128) for h in range(2)]
    for b in range(blocks):
        rows = pl.ds(128 * b, 128)
        rm[rows, :] = jnp.broadcast_to(mean_v[rows].reshape(1, 128), (128, 128)).T
        rs[rows, :] = jnp.broadcast_to(scale_v[rows].reshape(1, 128), (128, 128)).T
    pl.semaphore_wait(barrier, len(near))
    halo = pltpu.make_async_remote_copy(hs, hr, halo_sem.at[0], halo_sem.at[1], device_id=nxt, device_id_type=MESH)
    halo.start()

    def far(step, k):
        for to in (rem(z + step, NZ), rem(z + NZ - step, NZ)):
            pl.semaphore_signal(far_sem.at[k], inc=1, device_id={"z": to}, device_id_type=MESH)

    far(NEAR, 0)

    in_ow.wait()
    for cp in in_cot:
        cp.wait()
    u = lax.dot_general(cot[...], ow[...], (((1,), (1,)), ((), ())), preferred_element_type=F32)
    for h in range(2):
        us[h, :, :] = u[:, 128 * h:128 * h + 128]

    def conv_rows(h, r0, rows):
        acc = jnp.zeros((rows, 128), F32)
        for k in range(taps):
            acc = acc + wt[h, k:k + 1, :] * gp[h, pl.ds(r0 + (HALO + 1 - taps + k), rows), :]
        cv[h, pl.ds(r0, rows), :] = acc

    def point_rows(r0, rows):
        sl = pl.ds(r0, rows)
        sums = []
        for h in range(2):
            n = (cv[h, sl, :] - rm[sl, :]) * rs[sl, :]
            a = n * gain[h]
            s = sigmoid(a)
            hid[sl, pl.ds(128 * h, 128)] = (a * s).astype(BF16)
            da = us[h, sl, :] * s * (1.0 + a * (1.0 - s))
            d = da * gain[h]
            dan = da * n
            gacc[h, :, :] += dan.reshape(rows // 8, 8, 128).sum(axis=0)
            nm[h, sl, :] = n
            dn[h, sl, :] = d
            sums.append((d, dan * gain[h]))
        s1[sl, :] = sums[0][0] + sums[1][0]
        s2[sl, :] = sums[0][1] + sums[1][1]

    gacc[...] = jnp.zeros_like(gacc)
    @pl.loop(0, 8)
    def _(i):
        conv_rows(rem(i, 2), pl.multiple_of(HALO + div(i, 2) * 88, 8), 88)
    pl.semaphore_wait(far_sem.at[0], 2)
    far(2 * NEAR, 1)

    @pl.loop(0, (length - HALO) // 32)
    def _(i):
        point_rows(pl.multiple_of(HALO + i * 32, 32), 32)

    def row_sums(lo, hi):
        for b in range(lo, hi):
            rows = pl.ds(128 * b, 128)
            ys[b, 0:1, :] = jnp.sum(s1[rows, :].T, axis=0, keepdims=True)
            ys[b, 1:2, :] = jnp.sum(s2[rows, :].T, axis=0, keepdims=True)
        cps = []
        for q in (2, 1, 3):
            cps.append(pltpu.make_async_remote_copy(
                ys.at[pl.ds(lo, hi - lo)], yr.at[y, pl.ds(lo, hi - lo)], y_ss.at[q, min(lo, 1)], y_rs.at[q, min(lo, 1)],
                device_id={"y": rem(y + q, NY)}, device_id_type=MESH))
            cps[-1].start()
        return cps
    y_late = row_sums(1, blocks)

    @pl.loop(0, NH // 2)
    def _(i):
        for e in range(2):
            r = 2 * i + e
            lanes = pl.ds(pl.multiple_of(rem(zh + r, NH) * 128, 128), 128)
            cot_t[pl.ds(pl.multiple_of(r * 128, 128), 128), :] = cot[:, lanes].T
    halo.wait_recv()
    first_dev = ((z * NX + x) * NC + c) == 0
    for h in range(2):
        got = hr[:, pl.ds(128 * h, 128)].astype(F32)
        gp[h, 0:HALO, :] = jnp.where(first_dev, jnp.zeros_like(got), got)
        conv_rows(h, 0, HALO)
    point_rows(0, HALO)
    y_first = row_sums(0, 1)
    yr[y] = ys[...]
    rows_c = 64 * 2 * HC
    c_cp = []
    for k in range(CHUNKS):
        w = lax.dot_general(
            cot_t[pl.ds((k + 1) % CHUNKS * rows_c, rows_c), :], hid[...], (((1,), (0,)), ((), ())), preferred_element_type=F32)
        for e in range(HC):
            for pz in range(2):
                for px in range(NX):
                    for pc in range(NC):
                        r = 64 * (2 * e + pz) + 16 * px + 8 * pc
                        for h in range(2):
                            w32[k, pc, pz, px, e, h, :, :] = w[r:r + 8, 128 * h:128 * h + 128]
        c_cp.append(pltpu.make_async_remote_copy(
            w32.at[k, 1 - c], wc.at[k], c_ss.at[k], c_rs.at[k], device_id={"c": 1 - c}, device_id_type=MESH))
        c_cp[-1].start()
    pl.semaphore_wait(far_sem.at[1], 2)
    far(4 * NEAR, 2)

    x_cp = [[], []]

    def x_phase(p):
        for k in (2 * p, 2 * p + 1):
            c_cp[k].wait_recv()
            for pz in range(2):
                @pl.loop(0, NX)
                def _(px):
                    v = (w32[k, c, pz, px] + wc[k, pz, px]).reshape(HC, 16, 128)
                    xs[p, pz, px, k % 2 * HC:(k % 2 + 1) * HC] = v.astype(BF16)
        for pz, px, q in wmates:
            x_cp[p].append(pltpu.make_async_remote_copy(
                xs.at[p, pz, px], xr.at[q, p], x_ss.at[q, p], x_rs.at[q, p],
                device_id=mate(pz, px, c), device_id_type=MESH))
            x_cp[p][-1].start()
    x_phase(0)

    inv = 1.0 / (NY * pv.shape[1])

    def d_conv(lo, hi):
        for b in range(lo, hi):
            rows = pl.ds(128 * b, 128)
            tot = ((yr[0, b] + yr[1, b]) + (yr[2, b] + yr[3, b])) * inv
            s1[rows, :] = jnp.broadcast_to(tot[0:1, :], (128, 128)).T
            s2[rows, :] = jnp.broadcast_to(tot[1:2, :], (128, 128)).T

        @pl.loop(lo * 4, hi * 4)
        def _(i):
            sl = pl.ds(pl.multiple_of(i * 32, 32), 32)
            for h in range(2):
                dcp[h, sl, :] = rs[sl, :] * (dn[h, sl, :] - s1[sl, :] - nm[h, sl, :] * s2[sl, :])

    def tap_rows(lo, hi, start):
        for h in range(2):
            def step(i, acc):
                acc = list(acc)
                for e in range(4):
                    r0 = pl.multiple_of(i * 32 + 8 * e, 8)
                    d = dcp[h, pl.ds(r0, 8), :]
                    for k in range(taps):
                        acc[k] = acc[k] + d * gp[h, pl.ds(r0 + (HALO + 1 - taps + k), 8), :]
                return tuple(acc)
            init = tuple(jnp.zeros((8, 128), F32) if start else kacc[h, k] for k in range(taps))
            acc = lax.fori_loop(lo * 4, hi * 4, step, init)
            for k in range(taps):
                if start:
                    kacc[h, k] = acc[k]
                else:
                    tp[k // 4, 4 * h + k % 4, :] = jnp.sum(acc[k], axis=0)
    for cp in y_late:
        cp.wait_recv()
    d_conv(1, blocks)
    tap_rows(1, blocks, True)
    for h in range(2):
        tp[taps // 4, 4 * h + taps % 4, :] = jnp.sum(gacc[h], axis=0)
    for cp in y_first:
        cp.wait_recv()
    d_conv(0, 1)
    dhalo = pltpu.make_async_remote_copy(
        dcp.at[:, pl.ds(0, HALO), :], dcp.at[:, pl.ds(length, HALO), :], dhalo_sem.at[0], dhalo_sem.at[1],
        device_id=prv, device_id_type=MESH)
    tap_rows(0, 1, False)
    t_cp = []
    for pz, px, q in owners:
        t_cp.append(pltpu.make_async_remote_copy(
            tp.at[pz * NX + px], tr.at[c, g_me], t_ss.at[q], t_rs.at[c, q], device_id=mate(pz, px, 1), device_id_type=MESH))
    for cp in t_cp[:-1]:
        cp.start()

    @pl.when(c == 0)
    def _():
        t_cp[-1].start()

    @pl.when(c == 1)
    def _():
        tr[c, g_me] = tp[g_me]
    dhalo.start()
    x_phase(1)

    def d_gated(h, r0, rows):
        acc = jnp.zeros((rows, 128), F32)
        for k in range(taps):
            acc = acc + wt[h, k:k + 1, :] * dcp[h, pl.ds(r0 + (taps - 1 - k), rows), :]
        sl, lanes = pl.ds(r0, rows), pl.ds(128 * h, 128)
        s = sg[h, sl, :]
        vg_o[sl, lanes] = (acc * s).astype(BF16)
        gg_o[sl, lanes] = (acc * pv[sl, lanes].astype(F32) * s * (1.0 - s)).astype(BF16)
    @pl.loop(0, 2 * ((length - HALO) // 32))
    def _(i):
        d_gated(rem(i, 2), pl.multiple_of(div(i, 2) * 32, 32), 32)

    def z_copy(src, dst, ss, rs_, d):
        return pltpu.make_async_remote_copy(
            src, dst, ss.at[d], rs_.at[d], device_id={"z": rem(z + 2 * d, NZ)}, device_id_type=MESH)

    by_distance = [NH // 2]
    for d in range(NH // 2 - 1, 0, -1):
        by_distance += [d, NH - d]

    def tree(parts):
        while len(parts) > 1:
            parts = [a + b for a, b in zip(parts[::2], parts[1::2])] + parts[len(parts) // 2 * 2:]
        return parts[0]

    def z_phase(p):
        for cp in x_cp[p]:
            cp.wait_recv()
        for k in (2 * p, 2 * p + 1):
            v = (w32[k, c, zp, x] + wc[k, zp, x]).reshape(HC, 16, 128)
            for q in range(2 * NX - 1):
                v = v + xr[q, p, k % 2 * HC:(k % 2 + 1) * HC].astype(F32)
            r0 = (k + 1) % CHUNKS * HC
            if r0 == 0:
                zo[...] = v[0]
            zs[r0:r0 + HC] = v.astype(BF16)
        for d in by_distance:
            if (HC <= d < 3 * HC) == (p == 0):
                z_copy(zs.at[d], zr.at[d], z_ss, z_rs, d).start()
    pl.semaphore_wait(far_sem.at[2], 2)


    @pl.when(c == 1)
    def _():
        for pz, px, q in owners:
            for pc in range(NC):
                if q or pc == 0:
                    pltpu.make_async_remote_copy(
                        tp.at[0], tr.at[pc, 0], t_ss.at[q], t_rs.at[pc, q], device_id=mate(pz, px, 1), device_id_type=MESH
                    ).wait_recv()
        share = tree([tr[pc, g] for pc in range(NC) for g in range(2 * NX)])
        tf[0] = share
        for d in by_distance:
            z_copy(tf.at[0], tz.at[zh], tz_ss, tz_rs, d).start()
        tz[zh] = share
    z_phase(0)
    z_phase(1)
    last_dev = ((z * NX + x) * NC + c) == NZ * NX * NC - 1
    dhalo.wait_recv()
    for h in range(2):
        got = dcp[h, pl.ds(length, HALO), :]
        dcp[h, pl.ds(length, HALO), :] = jnp.where(last_dev, jnp.zeros_like(got), got)
        d_gated(h, length - HALO, HALO)

    halo.wait_send()
    dhalo.wait_send()
    for cp in y_late + y_first + c_cp + x_cp[0] + x_cp[1] + t_cp[:-1]:
        cp.wait_send()

    @pl.when(c == 0)
    def _():
        t_cp[-1].wait_send()

    def f_copy(q, to):
        return pltpu.make_async_remote_copy(
            tf.at[1], tacc.at[g_me], tf_ss.at[q], tf_rs.at[q], device_id=mate(*to), device_id_type=MESH)

    @pl.when(c == 1)
    def _():
        for d in range(1, NH):
            z_copy(tf.at[0], tz.at[zh], tz_ss, tz_rs, d).wait_recv()
        total = tree([tz[i] for i in range(NH)])
        tf[1] = total
        for q, to in enumerate(mates):
            f_copy(q, to).start()
        tacc[g_me] = total

    for d in range(1, NH):
        z_copy(zs.at[d], zr.at[d], z_ss, z_rs, d).wait_recv()
    wsum = tree([zo[...]] + [zr[i].astype(F32) for i in range(1, NH)])
    for h in range(2):
        wg_o[:, pl.ds(128 * h, 128)] = wsum[8 * h:8 * h + 8, :]
    for d in range(1, NH):
        z_copy(zs.at[d], zr.at[d], z_ss, z_rs, d).wait_send()

    @pl.when(c == 1)
    def _():
        for d in range(1, NH):
            z_copy(tf.at[0], tz.at[zh], tz_ss, tz_rs, d).wait_send()

    for q, (dx, dz, dc) in enumerate(steps):
        @pl.when(rem(c + dc, 2) == 1)
        def _():
            f_copy(q, mates[q]).wait_recv()
    for k in range(taps + 1):
        for h in range(2):
            row = tacc[k // 4, 4 * h + k % 4:4 * h + k % 4 + 1, :]
            if k < taps:
                tg_o[k:k + 1, pl.ds(128 * h, 128)] = row
            else:
                gn_o[pl.ds(128 * h, 128)] = row.reshape(128)

    @pl.when(c == 1)
    def _():
        for q, to in enumerate(mates):
            f_copy(q, to).wait_send()


def out_kernel(*refs):
    n = len(refs) // 2
    sems = refs[-1]
    cps = [pltpu.make_async_copy(refs[k], refs[n + k], sems.at[k]) for k in range(n)]
    for cp in cps:
        cp.start()
    for cp in cps:
        cp.wait()


def shards(pv, pg, cot, ow, taps, gain, mean, scale):
    length, ch = pv.shape
    d = cot.shape[1]
    blocks = length // 128
    V, D = pltpu.VMEM, pltpu.SemaphoreType.DMA
    any_spec, vmem = pl.BlockSpec(memory_space=pl.ANY), pl.BlockSpec(memory_space=pltpu.VMEM)
    scratch = [
        V((length, ch), BF16), V((length, ch), BF16), V((length, d), BF16), V((ch, d), BF16),
        V(taps.shape, BF16), V((ch,), F32), V((length,), F32), V((length,), F32),
        V((HALO, ch), BF16), V((HALO, ch), BF16),
        V((2, length + HALO, 128), F32), V((2, length, 128), F32), V((2, length, 128), F32),
        V((2, length, 128), F32), V((2, length, 128), F32), V((2, length, 128), F32),
        V((length, ch), BF16), V((2, length + HALO, 128), F32),
        V((length, 128), F32), V((length, 128), F32), V((length, 128), F32), V((length, 128), F32),
        V((2, 32, 128), F32), V((2, 8, 128), F32),
        V((d, length), BF16),
        V((blocks, 2, 128), F32), V((NY, blocks, 2, 128), F32),
        V((2, 32, 8, 128), F32),
        V((8, 8, 128), F32), V((8, 8, 128), F32), V((NC, 8, 8, 128), F32), V((NH, 8, 128), F32), V((2, 8, 128), F32),
        V((CHUNKS, NC, 2, NX, HC, 2, 8, 128), F32), V((CHUNKS, 2, NX, HC, 2, 8, 128), F32),
        V((2, 2, NX, NH // 2, 16, 128), BF16), V((2 * NX - 1, 2, NH // 2, 16, 128), BF16),
        V((NH, 16, 128), BF16), V((16, 128), F32), V((NH, 16, 128), BF16),
        D((10,)), D((2,)), D((2,)), D((NY, 2)), D((NY, 2)), D((8,)), D((NC, 8)), D((NH,)), D((NH,)), D((15,)), D((15,)),
        D((CHUNKS,)), D((CHUNKS,)), D((2 * NX - 1, 2)), D((2 * NX - 1, 2)), D((NH,)), D((NH,)),
        pltpu.SemaphoreType.REGULAR((3,)),
    ]
    outs = (((length, ch), BF16), ((length, ch), BF16), ((8, ch), F32), (taps.shape, F32), ((ch,), F32))
    res = pl.pallas_call(
        main_kernel,
        out_shape=tuple(V(s, t) for s, t in outs),
        in_specs=[any_spec] * 8,
        out_specs=(vmem,) * 5,
        scratch_shapes=scratch,
        name="conv_back",
        compiler_params=pltpu.CompilerParams(collective_id=0, has_side_effects=True, vmem_limit_bytes=56 * 2**20),
    )(pv, pg, cot, ow, taps, gain, mean, scale)
    return pl.pallas_call(
        out_kernel,
        out_shape=tuple(jax.ShapeDtypeStruct(s, t) for s, t in outs),
        in_specs=[vmem] * 5,
        out_specs=(any_spec,) * 5,
        scratch_shapes=[D((5,))],
        name="write_out",
    )(*(pltpu.with_memory_space_constraint(r, pltpu.VMEM) for r in res))


def solution(mesh):
    split = Mesh(mesh.devices.reshape(NZ, NX, NC, mesh.shape["tp"]), ("z", "x", "c", "y"))
    placed = (P(SP, "y"), P(SP, "y"), P(SP, None), P("y", None), P(None, "y"), P("y"), P(SP), P(SP))
    return jax.shard_map(
        shards, mesh=split, in_specs=placed,
        out_specs=(P(SP, "y"), P(SP, "y"), P(SP, "y"), P(None, "y"), P("y")), check_vma=False,
    )
```

```python
import functools

import jax
import jax.numpy as jnp
from jax import lax
from jax.experimental import pallas as pl
from jax.experimental.pallas import tpu as pltpu
from jax.sharding import Mesh
from jax.sharding import PartitionSpec as P

MESH = pl.DeviceIdType.MESH
SP = ("z", "x", "c")
NZ, NX, NC, NY = 32, 4, 2, 4
F32, BF16 = jnp.float32, jnp.bfloat16
HALO = 32
NH = NZ // 2
CHUNKS = 4
HC = NH // CHUNKS


def sigmoid(v):
    return 1.0 / (1.0 + jnp.exp(-v))


def main_kernel(
    pv_h, pg_h, cot_h, ow_h, taps_h, gain_h, mean_h, scale_h,
    vg_o, gg_o, wg_o, tg_o, gn_o,
    pvg, cot, ow, taps_b, gain_v, mean_v, scale_v,
    hs, hr, gp, sg, us, cv, nm, dn, hid, dcp, rm, rs, s1, s2, wt, gacc,
    cot_t, ys, yr, ys0, yr0, kacc, tacc, tp, tr, tz, tf, w32, wc, xs, xr, zs, zr,
    in_sem, halo_sem, dhalo_sem, y_ss, y_rs, t_ss, t_rs, tz_ss, tz_rs, tf_ss, tf_rs,
    c_ss, c_rs, x_ss, x_rs, z_ss, z_rs, far_sem,
):
    length = pvg.shape[1]
    taps = taps_b.shape[0]
    blocks = length // 128
    z, x, c, y = (lax.axis_index(a) for a in ("z", "x", "c", "y"))
    rem, div = lax.rem, lax.div
    zh, zp = div(z, 2), rem(z, 2)
    g_me, g_sum = zp * NX + x, (1 - zp) * NX + x

    def copy_in(src, dst, k):
        cp = pltpu.make_async_copy(src, dst, in_sem.at[k])
        cp.start()
        return cp

    def wait_for(ref, sem):
        pltpu.make_async_copy(ref, ref, sem).wait()

    copy_in(pv_h, pvg.at[0], 0)
    copy_in(pg_h, pvg.at[1], 0)
    in_small = [copy_in(s, d, 1 + k) for k, (s, d) in enumerate(
        ((taps_h, taps_b), (gain_h, gain_v), (mean_h, mean_v), (scale_h, scale_v)))]
    rows_w = cot.shape[0] // 6
    for src, dst, sem in ((ow_h, ow, 5), (cot_h, cot, 6)):
        for k in range(dst.shape[0] // rows_w):
            rows = pl.ds(rows_w * k, rows_w)
            copy_in(src.at[rows, :], dst.at[rows, :], sem)

    steps = [(dx, dz, dc) for dx in (2, 1, 3, 0) for dz in range(2) for dc in range(NC) if dx or dz or dc]
    mates = [(rem(zp + dz, 2), rem(x + dx, NX), rem(c + dc, NC)) for dx, dz, dc in steps]
    owners = []
    for dx in (2, 1, 3, 0):
        for dz in (1, 0):
            owners.append((rem(zp + dz, 2), rem(x + dx, NX), dz * NX + dx))
    wmates = []
    for dx in (2, 1, 3, 0):
        for dz in range(2):
            if dx or dz:
                wmates.append((rem(zp + dz, 2), rem(x + dx, NX), dz * NX + dx - 1))

    def mate(pz, px, pc):
        return {"z": 2 * zh + pz, "x": px, "c": pc}

    nxt = {"z": rem(z + div(x * NC + c + 1, NX * NC), NZ), "x": rem(x + c, NX), "c": 1 - c}
    prv = {"z": rem(z + NZ - 1 + div(x + NX - 1 + c, NX), NZ), "x": rem(x + NX - 1 + c, NX), "c": 1 - c}
    barrier = pltpu.get_barrier_semaphore()

    def along(axis, size, step):
        me = lax.axis_index(axis)
        return [{axis: rem(me + step, size)}, {axis: rem(me + size - step, size)}]

    core, x1, y1, z1, z2 = [{"c": 1 - c}], along("x", NX, 1), along("y", NY, 1), along("z", NZ, 1), along("z", NZ, 2)
    entry = z2 + [prv, nxt] + x1 + y1 + along("y", NY, 2)[:1] + z1 + core
    for to in entry:
        pl.semaphore_signal(barrier, inc=1, device_id=to, device_id_type=MESH)

    stages = [z2 + core + x1 + y1 + z1, along("z", NZ, 4) + core + along("x", NX, 2)[:1], along("z", NZ, 8)]

    def tell(k):
        for to in stages[k]:
            pl.semaphore_signal(far_sem.at[k], inc=1, device_id=to, device_id_type=MESH)

    def heard(k):
        pl.semaphore_wait(far_sem.at[k], len(stages[k]))

    gacc[...] = jnp.zeros_like(gacc)
    for part in (s1, s2):
        part[0:HALO, :] = jnp.zeros((HALO, 128), F32)

    wait_for(pvg, in_sem.at[0])

    def gate_rows(r0, rows):
        for h in range(2):
            lanes = pl.ds(128 * h, 128)
            s = sigmoid(pvg[1, pl.ds(r0, rows), lanes].astype(F32))
            g = (pvg[0, pl.ds(r0, rows), lanes].astype(F32) * s).astype(BF16)
            sg[h, pl.ds(r0, rows), :] = s
            gp[h, pl.ds(r0 + HALO, rows), :] = g.astype(F32)
            yield lanes, g
    for lanes, g in gate_rows(length - HALO, HALO):
        hs[:, lanes] = g

    @pl.loop(0, (length - HALO) // 32)
    def _(i):
        for _ in gate_rows(pl.multiple_of(i * 32, 32), 32):
            pass

    for cp in in_small:
        cp.wait()
    for h in range(2):
        wt[h, 0:taps, :] = taps_b[:, pl.ds(128 * h, 128)].astype(F32)
    gain = [gain_v[pl.ds(128 * h, 128)].reshape(1, 128) for h in range(2)]
    for b in range(blocks):
        rows = pl.ds(128 * b, 128)
        rm[rows, :] = jnp.broadcast_to(mean_v[rows].reshape(1, 128), (128, 128)).T
        rs[rows, :] = jnp.broadcast_to(scale_v[rows].reshape(1, 128), (128, 128)).T
    pl.semaphore_wait(barrier, len(entry))
    halo = pltpu.make_async_remote_copy(hs, hr, halo_sem.at[0], halo_sem.at[1], device_id=nxt, device_id_type=MESH)
    halo.start()
    tell(0)

    def conv_rows(h, r0, rows):
        acc = jnp.zeros((rows, 128), F32)
        for k in range(taps):
            acc = acc + wt[h, k:k + 1, :] * gp[h, pl.ds(r0 + (HALO + 1 - taps + k), rows), :]
        cv[h, pl.ds(r0, rows), :] = acc

    def point_rows(r0, rows):
        sl = pl.ds(r0, rows)
        sums = []
        for h in range(2):
            n = (cv[h, sl, :] - rm[sl, :]) * rs[sl, :]
            a = n * gain[h]
            s = sigmoid(a)
            hid[sl, pl.ds(128 * h, 128)] = (a * s).astype(BF16)
            da = us[h, sl, :] * s * (1.0 + a * (1.0 - s))
            d = da * gain[h]
            dan = da * n
            gacc[h, :, :] += dan.reshape(rows // 8, 8, 128).sum(axis=0)
            nm[h, sl, :] = n
            dn[h, sl, :] = d
            sums.append((d, dan * gain[h]))
        s1[sl, :] = sums[0][0] + sums[1][0]
        s2[sl, :] = sums[0][1] + sums[1][1]
    @pl.loop(0, 8)
    def _(i):
        conv_rows(rem(i, 2), pl.multiple_of(HALO + div(i, 2) * 88, 8), 88)
    wait_for(ow, in_sem.at[5])
    wait_for(cot, in_sem.at[6])
    u = lax.dot_general(cot[...], ow[...], (((1,), (1,)), ((), ())), preferred_element_type=F32)
    for h in range(2):
        us[h, :, :] = u[:, 128 * h:128 * h + 128]
    @pl.loop(0, (length - HALO) // 32)
    def _(i):
        point_rows(pl.multiple_of(HALO + i * 32, 32), 32)

    def row_sums(lo, hi, part, ys, yr):
        for b in range(lo, hi):
            rows = pl.ds(128 * b, 128)
            ys[b, 0:1, :] = jnp.sum(s1[rows, :].T, axis=0, keepdims=True)
            ys[b, 1:2, :] = jnp.sum(s2[rows, :].T, axis=0, keepdims=True)
        cps = []
        for q in (2, 1, 3):
            cps.append(pltpu.make_async_remote_copy(
                ys, yr.at[y], y_ss.at[part], y_rs.at[part], device_id={"y": rem(y + q, NY)}, device_id_type=MESH))
            cps[-1].start()
        return cps
    y_late = row_sums(0, blocks, 0, ys, yr)
    yr[y] = ys[...]
    heard(0)
    tell(1)

    @pl.loop(0, NH // 2)
    def _(i):
        for e in range(2):
            r = 2 * i + e
            lanes = pl.ds(pl.multiple_of(rem(zh + r, NH) * 128, 128), 128)
            cot_t[pl.ds(pl.multiple_of(r * 128, 128), 128), :] = cot[:, lanes].T
    halo.wait_recv()
    first_dev = ((z * NX + x) * NC + c) == 0
    for h in range(2):
        got = hr[:, pl.ds(128 * h, 128)].astype(F32)
        gp[h, 0:HALO, :] = jnp.where(first_dev, jnp.zeros_like(got), got)
        conv_rows(h, 0, HALO)
    point_rows(0, HALO)
    y_first = row_sums(0, 1, 1, ys0, yr0)
    yr0[y] = ys0[...]
    rows_c = 64 * 2 * HC

    def c_copy(k):
        return pltpu.make_async_remote_copy(
            w32.at[k, 1 - c], wc.at[k], c_ss, c_rs.at[div(k, 2)], device_id={"c": 1 - c}, device_id_type=MESH)

    @pl.loop(0, CHUNKS)
    def _(k):
        rows = pl.ds(pl.multiple_of(rem(k + 1, CHUNKS) * rows_c, rows_c), rows_c)
        w = lax.dot_general(cot_t[rows, :], hid[...], (((1,), (0,)), ((), ())), preferred_element_type=F32)
        for e in range(HC):
            for pz in range(2):
                for px in range(NX):
                    for pc in range(NC):
                        r = 64 * (2 * e + pz) + 16 * px + 8 * pc
                        for h in range(2):
                            w32[k, pc, pz, px, e, h, :, :] = w[r:r + 8, 128 * h:128 * h + 128]
        c_copy(k).start()

    x_cp = [[pltpu.make_async_remote_copy(
        xs.at[p, 1 - pz, px], xr.at[p, q], x_ss.at[p], x_rs.at[p], device_id=mate(pz, px, c), device_id_type=MESH)
        for pz, px, q in wmates] for p in range(2)]

    def x_phase(p):
        wait_for(wc.at[pl.ds(2 * p, 2)], c_rs.at[p])
        for k in (2 * p, 2 * p + 1):
            for pz in range(2):
                @pl.loop(0, NX)
                def _(px):
                    v = (w32[k, c, pz, px] + wc[k, pz, px]).reshape(HC, 16, 128)
                    xs[p, pz, px, k % 2 * HC:(k % 2 + 1) * HC] = v.astype(BF16)
        for cp in x_cp[p]:
            cp.start()
    heard(1)
    tell(2)
    inv = 1.0 / (NY * pvg.shape[2])

    def d_conv(lo, hi, yr):
        for b in range(lo // 4, (hi + 3) // 4):
            rows = pl.ds(128 * b, 128)
            tot = ((yr[0, b] + yr[1, b]) + (yr[2, b] + yr[3, b])) * inv
            s1[rows, :] = jnp.broadcast_to(tot[0:1, :], (128, 128)).T
            s2[rows, :] = jnp.broadcast_to(tot[1:2, :], (128, 128)).T

        @pl.loop(lo, hi)
        def _(i):
            sl = pl.ds(pl.multiple_of(i * 32, 32), 32)
            for h in range(2):
                dcp[h, sl, :] = rs[sl, :] * (dn[h, sl, :] - s1[sl, :] - nm[h, sl, :] * s2[sl, :])

    def tap_rows(lo, hi, start):
        for h in range(2):
            def step(i, acc):
                acc = list(acc)
                for e in range(4):
                    r0 = pl.multiple_of(i * 32 + 8 * e, 8)
                    d = dcp[h, pl.ds(r0, 8), :]
                    for k in range(taps):
                        acc[k] = acc[k] + d * gp[h, pl.ds(r0 + (HALO + 1 - taps + k), 8), :]
                return tuple(acc)
            init = tuple(jnp.zeros((8, 128), F32) if start else kacc[h, k] for k in range(taps))
            acc = lax.fori_loop(lo, hi, step, init)
            for k in range(taps):
                if start:
                    kacc[h, k] = acc[k]
                else:
                    tp[k // 4, 4 * h + k % 4, :] = jnp.sum(acc[k], axis=0)
    wait_for(yr.at[pl.ds(0, NY - 1)], y_rs.at[0])
    d_conv(1, length // 32, yr)
    tap_rows(1, length // 32, True)
    for h in range(2):
        tp[taps // 4, 4 * h + taps % 4, :] = jnp.sum(gacc[h], axis=0)
    wait_for(yr0.at[pl.ds(0, NY - 1)], y_rs.at[1])
    d_conv(0, 1, yr0)
    dhalo = pltpu.make_async_remote_copy(
        dcp.at[:, pl.ds(0, HALO), :], dcp.at[:, pl.ds(length, HALO), :], dhalo_sem.at[0], dhalo_sem.at[1],
        device_id=prv, device_id_type=MESH)
    tap_rows(0, 1, False)
    t_cp = []
    for pz, px, q in owners:
        t_cp.append(pltpu.make_async_remote_copy(
            tp.at[pz * NX + px], tr.at[8 * c + g_me], t_ss, t_rs, device_id=mate(pz, px, 1), device_id_type=MESH))
    for cp in t_cp[:-1]:
        cp.start()

    @pl.when(c == 0)
    def _():
        t_cp[-1].start()

    @pl.when(c == 1)
    def _():
        tr[8 * c + g_me] = tp[g_me]
    dhalo.start()
    x_phase(0)
    x_phase(1)

    def d_gated(h, r0, rows):
        acc = jnp.zeros((rows, 128), F32)
        for k in range(taps):
            acc = acc + wt[h, k:k + 1, :] * dcp[h, pl.ds(r0 + (taps - 1 - k), rows), :]
        sl, lanes = pl.ds(r0, rows), pl.ds(128 * h, 128)
        s = sg[h, sl, :]
        vg_o[sl, lanes] = (acc * s).astype(BF16)
        gg_o[sl, lanes] = (acc * pvg[0, sl, lanes].astype(F32) * s * (1.0 - s)).astype(BF16)
    @pl.loop(0, 2 * ((length - HALO) // 32))
    def _(i):
        d_gated(rem(i, 2), pl.multiple_of(div(i, 2) * 32, 32), 32)

    def z_copy(src, dst, ss, rs_, d):
        return pltpu.make_async_remote_copy(
            src, dst, ss, rs_, device_id={"z": rem(z + 2 * d + 1 + 2 * (NH - 1) * zp, NZ)}, device_id_type=MESH)

    by_distance = []
    for d in range(NH // 2 - 1, -1, -1):
        by_distance += [NH - 1 - d, d]

    def tree(parts):
        while len(parts) > 1:
            parts = [a + b for a, b in zip(parts[::2], parts[1::2])] + parts[len(parts) // 2 * 2:]
        return parts[0]

    def z_phase(p):
        wait_for(xr.at[p], x_rs.at[p])
        for k in (2 * p, 2 * p + 1):
            v = (w32[k, c, 1 - zp, x] + wc[k, 1 - zp, x]).reshape(HC, 16, 128)
            for q in range(2 * NX - 1):
                v = v + xr[p, q, k % 2 * HC:(k % 2 + 1) * HC].astype(F32)
            r0 = (k + 1) % CHUNKS * HC
            zs[r0:r0 + HC] = v.astype(BF16)
        for d in by_distance:
            if (HC <= d < 3 * HC) == (p == 0):
                z_copy(zs.at[d], zr.at[d], z_ss, z_rs, d).start()
    heard(2)


    @pl.when(c == 1)
    def _():
        wait_for(tr.at[pl.ds(0, 15)], t_rs)
        share = tree([tr[k] for k in range(16)])
        tf[0] = share
        for d in by_distance:
            z_copy(tf.at[0], tz.at[zh], tz_ss, tz_rs, d).start()
    z_phase(0)
    z_phase(1)
    last_dev = ((z * NX + x) * NC + c) == NZ * NX * NC - 1
    dhalo.wait_recv()
    for h in range(2):
        got = dcp[h, pl.ds(length, HALO), :]
        dcp[h, pl.ds(length, HALO), :] = jnp.where(last_dev, jnp.zeros_like(got), got)
        d_gated(h, length - HALO, HALO)

    halo.wait_send()
    dhalo.wait_send()
    wait_for(yr.at[pl.ds(0, NY - 1)], y_ss.at[0])
    wait_for(yr0.at[pl.ds(0, NY - 1)], y_ss.at[1])
    wait_for(wc, c_ss)
    for p in range(2):
        wait_for(xr.at[p], x_ss.at[p])

    @pl.when(c == 0)
    def _():
        wait_for(tp, t_ss)

    @pl.when(c == 1)
    def _():
        wait_for(tp.at[pl.ds(0, 7)], t_ss)

    def f_copy(to):
        return pltpu.make_async_remote_copy(
            tf.at[1], tacc.at[g_sum], tf_ss, tf_rs, device_id=mate(*to), device_id_type=MESH)

    @pl.when(c == 1)
    def _():
        wait_for(tz, tz_rs)
        total = tree([tz[i] for i in range(NH)])
        tf[1] = total
        for to in mates:
            f_copy(to).start()
        tacc[g_sum] = total

    wait_for(zr, z_rs)
    wsum = tree([zr[i].astype(F32) for i in range(NH)])
    for h in range(2):
        wg_o[:, pl.ds(128 * h, 128)] = wsum[8 * h:8 * h + 8, :]
    wait_for(zr, z_ss)

    @pl.when(c == 1)
    def _():
        wait_for(tz, tz_ss)

    @pl.when(c == 0)
    def _():
        wait_for(tacc, tf_rs)

    @pl.when(c == 1)
    def _():
        wait_for(tacc.at[pl.ds(0, 7)], tf_rs)
    for k in range(taps + 1):
        for h in range(2):
            row = tacc[k // 4, 4 * h + k % 4:4 * h + k % 4 + 1, :]
            if k < taps:
                tg_o[k:k + 1, pl.ds(128 * h, 128)] = row
            else:
                gn_o[pl.ds(128 * h, 128)] = row.reshape(128)

    @pl.when(c == 1)
    def _():
        wait_for(tr.at[pl.ds(0, 15)], tf_ss)


def out_kernel(*refs):
    n = len(refs) // 2
    sems = refs[-1]
    cps = [pltpu.make_async_copy(refs[k], refs[n + k], sems.at[k]) for k in range(n)]
    for cp in cps:
        cp.start()
    for cp in cps:
        cp.wait()


def shards(pv, pg, cot, ow, taps, gain, mean, scale):
    length, ch = pv.shape
    d = cot.shape[1]
    blocks = length // 128
    V, D = pltpu.VMEM, pltpu.SemaphoreType.DMA
    any_spec, vmem = pl.BlockSpec(memory_space=pl.ANY), pl.BlockSpec(memory_space=pltpu.VMEM)
    scratch = [
        V((2, length, ch), BF16), V((length, d), BF16), V((ch, d), BF16),
        V(taps.shape, BF16), V((ch,), F32), V((length,), F32), V((length,), F32),
        V((HALO, ch), BF16), V((HALO, ch), BF16),
        V((2, length + HALO, 128), F32), V((2, length, 128), F32), V((2, length, 128), F32),
        V((2, length, 128), F32), V((2, length, 128), F32), V((2, length, 128), F32),
        V((length, ch), BF16), V((2, length + HALO, 128), F32),
        V((length, 128), F32), V((length, 128), F32), V((length, 128), F32), V((length, 128), F32),
        V((2, 32, 128), F32), V((2, 8, 128), F32),
        V((d, length), BF16),
        V((blocks, 2, 128), F32), V((NY, blocks, 2, 128), F32), V((1, 2, 128), F32), V((NY, 1, 2, 128), F32),
        V((2, 32, 8, 128), F32),
        V((8, 8, 128), F32), V((8, 8, 128), F32), V((16, 8, 128), F32), V((NH, 8, 128), F32), V((2, 8, 128), F32),
        V((CHUNKS, NC, 2, NX, HC, 2, 8, 128), F32), V((CHUNKS, 2, NX, HC, 2, 8, 128), F32),
        V((2, 2, NX, NH // 2, 16, 128), BF16), V((2, 2 * NX - 1, NH // 2, 16, 128), BF16),
        V((NH, 16, 128), BF16), V((NH, 16, 128), BF16),
        D((7,)), D((2,)), D((2,)), D((2,)), D((2,)), D, D, D, D, D, D,
        D, D((2,)), D((2,)), D((2,)), D, D,
        pltpu.SemaphoreType.REGULAR((3,)),
    ]
    outs = (((length, ch), BF16), ((length, ch), BF16), ((8, ch), F32), (taps.shape, F32), ((ch,), F32))
    res = pl.pallas_call(
        main_kernel,
        out_shape=tuple(V(s, t) for s, t in outs),
        in_specs=[any_spec] * 8,
        out_specs=(vmem,) * 5,
        scratch_shapes=scratch,
        name="conv_back",
        compiler_params=pltpu.CompilerParams(collective_id=0, has_side_effects=True, vmem_limit_bytes=56 * 2**20),
    )(pv, pg, cot, ow, taps, gain, mean, scale)
    return pl.pallas_call(
        out_kernel,
        out_shape=tuple(jax.ShapeDtypeStruct(s, t) for s, t in outs),
        in_specs=[vmem] * 5,
        out_specs=(any_spec,) * 5,
        scratch_shapes=[D((5,))],
        name="write_out",
    )(*(pltpu.with_memory_space_constraint(r, pltpu.VMEM) for r in res))


def solution(mesh):
    split = Mesh(mesh.devices.reshape(NZ, NX, NC, mesh.shape["tp"]), ("z", "x", "c", "y"))
    placed = (P(SP, "y"), P(SP, "y"), P(SP, None), P("y", None), P(None, "y"), P("y"), P(SP), P(SP))
    return jax.shard_map(
        shards, mesh=split, in_specs=placed,
        out_specs=(P(SP, "y"), P(SP, "y"), P(SP, "y"), P(None, "y"), P("y")), check_vma=False,
    )
```

```python
import functools

import jax
import jax.numpy as jnp
from jax import lax
from jax.experimental import pallas as pl
from jax.experimental.pallas import tpu as pltpu
from jax.sharding import Mesh
from jax.sharding import PartitionSpec as P

MESH = pl.DeviceIdType.MESH
SP = ("z", "x", "c")
NZ, NX, NC, NY = 32, 4, 2, 4
F32, BF16 = jnp.float32, jnp.bfloat16
HALO = 32
NH = NZ // 2
CHUNKS = 4
HC = NH // CHUNKS
EARLY, FIRST = 12, 2 * HC


def sigmoid(v):
    return 1.0 / (1.0 + jnp.exp(-v))


def main_kernel(
    pv_h, pg_h, cot_h, ow_h, taps_h, gain_h, mean_h, scale_h,
    vg_o, gg_o, wg_o, tg_o, gn_o,
    pvg, cot, ow, taps_b, gain_v, mean_v, scale_v,
    hs, hr, gp, sg, us, cv, nm, dn, hid, dcp, rm, rs, s1, s2, wt, gacc,
    cot_t, ys, yr, ys0, yr0, kacc, tacc, tp, tr, tz, tf, w32, wc, xs0, xs1, xr0, xr1, zs, zr,
    in_sem, halo_sem, dhalo_sem, y_ss, y_rs, t_ss, t_rs, tz_ss, tz_rs, tf_ss, tf_rs,
    c_ss, c_rs, x_ss, x_rs, z_ss, z_rs, far_sem,
):
    length = pvg.shape[1]
    taps = taps_b.shape[0]
    blocks = length // 128
    z, x, c, y = (lax.axis_index(a) for a in ("z", "x", "c", "y"))
    rem, div = lax.rem, lax.div
    zh, zp = div(z, 2), rem(z, 2)
    g_me, g_sum = zp * NX + x, (1 - zp) * NX + x

    def copy_in(src, dst, k):
        cp = pltpu.make_async_copy(src, dst, in_sem.at[k])
        cp.start()
        return cp

    def wait_for(ref, sem):
        pltpu.make_async_copy(ref, ref, sem).wait()

    copy_in(pv_h, pvg.at[0], 0)
    copy_in(pg_h, pvg.at[1], 0)
    in_small = [copy_in(s, d, 1 + k) for k, (s, d) in enumerate(
        ((taps_h, taps_b), (gain_h, gain_v), (mean_h, mean_v), (scale_h, scale_v)))]
    rows_w = cot.shape[0] // 6
    for src, dst, sem in ((ow_h, ow, 5), (cot_h, cot, 6)):
        for k in range(dst.shape[0] // rows_w):
            rows = pl.ds(rows_w * k, rows_w)
            copy_in(src.at[rows, :], dst.at[rows, :], sem)

    steps = [(dx, dz, dc) for dx in (2, 1, 3, 0) for dz in range(2) for dc in range(NC) if dx or dz or dc]
    mates = [(rem(zp + dz, 2), rem(x + dx, NX), rem(c + dc, NC)) for dx, dz, dc in steps]
    owners = []
    for dx in (2, 1, 3, 0):
        for dz in (1, 0):
            owners.append((rem(zp + dz, 2), rem(x + dx, NX), dz * NX + dx))
    wmates = []
    for dx in (2, 1, 3, 0):
        for dz in range(2):
            if dx or dz:
                wmates.append((rem(zp + dz, 2), rem(x + dx, NX), dz * NX + dx - 1))

    def mate(pz, px, pc):
        return {"z": 2 * zh + pz, "x": px, "c": pc}

    nxt = {"z": rem(z + div(x * NC + c + 1, NX * NC), NZ), "x": rem(x + c, NX), "c": 1 - c}
    prv = {"z": rem(z + NZ - 1 + div(x + NX - 1 + c, NX), NZ), "x": rem(x + NX - 1 + c, NX), "c": 1 - c}
    barrier = pltpu.get_barrier_semaphore()

    def along(axis, size, step):
        me = lax.axis_index(axis)
        return [{axis: rem(me + step, size)}, {axis: rem(me + size - step, size)}]

    core, x1, y1, z1, z2 = [{"c": 1 - c}], along("x", NX, 1), along("y", NY, 1), along("z", NZ, 1), along("z", NZ, 2)
    entry = z2 + [prv, nxt] + x1 + y1 + along("y", NY, 2)[:1] + z1 + core
    for to in entry:
        pl.semaphore_signal(barrier, inc=1, device_id=to, device_id_type=MESH)

    stages = [z2 + core + x1 + y1 + z1, along("z", NZ, 4) + core + along("x", NX, 2)[:1], along("z", NZ, 8)]

    def tell(k):
        for to in stages[k]:
            pl.semaphore_signal(far_sem.at[k], inc=1, device_id=to, device_id_type=MESH)

    def heard(k):
        pl.semaphore_wait(far_sem.at[k], len(stages[k]))

    gacc[...] = jnp.zeros_like(gacc)
    for part in (s1, s2):
        part[0:HALO, :] = jnp.zeros((HALO, 128), F32)

    wait_for(pvg, in_sem.at[0])

    def gate_rows(r0, rows):
        for h in range(2):
            lanes = pl.ds(128 * h, 128)
            s = sigmoid(pvg[1, pl.ds(r0, rows), lanes].astype(F32))
            g = (pvg[0, pl.ds(r0, rows), lanes].astype(F32) * s).astype(BF16)
            sg[h, pl.ds(r0, rows), :] = s
            gp[h, pl.ds(r0 + HALO, rows), :] = g.astype(F32)
            yield lanes, g
    for lanes, g in gate_rows(length - HALO, HALO):
        hs[:, lanes] = g

    @pl.loop(0, (length - HALO) // 32)
    def _(i):
        for _ in gate_rows(pl.multiple_of(i * 32, 32), 32):
            pass

    for cp in in_small:
        cp.wait()
    for h in range(2):
        wt[h, 0:taps, :] = taps_b[:, pl.ds(128 * h, 128)].astype(F32)
    gain = [gain_v[pl.ds(128 * h, 128)].reshape(1, 128) for h in range(2)]
    for b in range(blocks):
        rows = pl.ds(128 * b, 128)
        rm[rows, :] = jnp.broadcast_to(mean_v[rows].reshape(1, 128), (128, 128)).T
        rs[rows, :] = jnp.broadcast_to(scale_v[rows].reshape(1, 128), (128, 128)).T
    pl.semaphore_wait(barrier, len(entry))
    halo = pltpu.make_async_remote_copy(hs, hr, halo_sem.at[0], halo_sem.at[1], device_id=nxt, device_id_type=MESH)
    halo.start()
    tell(0)

    def conv_rows(h, r0, rows):
        acc = jnp.zeros((rows, 128), F32)
        for k in range(taps):
            acc = acc + wt[h, k:k + 1, :] * gp[h, pl.ds(r0 + (HALO + 1 - taps + k), rows), :]
        cv[h, pl.ds(r0, rows), :] = acc

    def point_rows(r0, rows):
        sl = pl.ds(r0, rows)
        sums = []
        for h in range(2):
            n = (cv[h, sl, :] - rm[sl, :]) * rs[sl, :]
            a = n * gain[h]
            s = sigmoid(a)
            hid[sl, pl.ds(128 * h, 128)] = (a * s).astype(BF16)
            da = us[h, sl, :] * s * (1.0 + a * (1.0 - s))
            d = da * gain[h]
            dan = da * n
            gacc[h, :, :] += dan.reshape(rows // 8, 8, 128).sum(axis=0)
            nm[h, sl, :] = n
            dn[h, sl, :] = d
            sums.append((d, dan * gain[h]))
        s1[sl, :] = sums[0][0] + sums[1][0]
        s2[sl, :] = sums[0][1] + sums[1][1]
    @pl.loop(0, 8)
    def _(i):
        conv_rows(rem(i, 2), pl.multiple_of(HALO + div(i, 2) * 88, 8), 88)
    wait_for(ow, in_sem.at[5])
    wait_for(cot, in_sem.at[6])
    u = lax.dot_general(cot[...], ow[...], (((1,), (1,)), ((), ())), preferred_element_type=F32)
    for h in range(2):
        us[h, :, :] = u[:, 128 * h:128 * h + 128]
    @pl.loop(0, (length - HALO) // 32)
    def _(i):
        point_rows(pl.multiple_of(HALO + i * 32, 32), 32)

    def row_sums(lo, hi, part, ys, yr):
        for b in range(lo, hi):
            rows = pl.ds(128 * b, 128)
            ys[b, 0:1, :] = jnp.sum(s1[rows, :].T, axis=0, keepdims=True)
            ys[b, 1:2, :] = jnp.sum(s2[rows, :].T, axis=0, keepdims=True)
        cps = []
        for q in (2, 1, 3):
            cps.append(pltpu.make_async_remote_copy(
                ys, yr.at[y], y_ss.at[part], y_rs.at[part], device_id={"y": rem(y + q, NY)}, device_id_type=MESH))
            cps[-1].start()
        return cps
    y_late = row_sums(0, blocks, 0, ys, yr)
    yr[y] = ys[...]
    heard(0)
    tell(1)

    @pl.loop(0, NH // 2)
    def _(i):
        for e in range(2):
            r = 2 * i + e
            lanes = pl.ds(pl.multiple_of(r * 128, 128), 128)
            cot_t[pl.ds(pl.multiple_of(r * 128, 128), 128), :] = cot[:, lanes].T
    halo.wait_recv()
    first_dev = ((z * NX + x) * NC + c) == 0
    for h in range(2):
        got = hr[:, pl.ds(128 * h, 128)].astype(F32)
        gp[h, 0:HALO, :] = jnp.where(first_dev, jnp.zeros_like(got), got)
        conv_rows(h, 0, HALO)
    point_rows(0, HALO)
    y_first = row_sums(0, 1, 1, ys0, yr0)
    yr0[y] = ys0[...]
    rows_c = 64 * 2 * HC

    def c_copy(k):
        return pltpu.make_async_remote_copy(
            w32.at[k, 1 - c], wc.at[k], c_ss, c_rs.at[div(k + CHUNKS - 2, CHUNKS - 1)], device_id={"c": 1 - c}, device_id_type=MESH)

    @pl.loop(0, CHUNKS)
    def _(k):
        rows = pl.ds(pl.multiple_of(k * rows_c, rows_c), rows_c)
        w = lax.dot_general(cot_t[rows, :], hid[...], (((1,), (0,)), ((), ())), preferred_element_type=F32)
        for e in range(HC):
            for pz in range(2):
                for px in range(NX):
                    for pc in range(NC):
                        r = 64 * (2 * e + pz) + 16 * px + 8 * pc
                        for h in range(2):
                            w32[k, pc, pz, px, e, h, :, :] = w[r:r + 8, 128 * h:128 * h + 128]
        c_copy(k).start()

    parts = ((xs0, xr0, 0, 1), (xs1, xr1, 1, CHUNKS))
    x_cp = [[pltpu.make_async_remote_copy(
        xs.at[1 - pz, px], xr.at[q], x_ss.at[p], x_rs.at[p], device_id=mate(pz, px, c), device_id_type=MESH)
        for pz, px, q in wmates] for p, (xs, xr, _, _) in enumerate(parts)]

    def x_phase(p):
        xs, xr, lo, hi = parts[p]
        wait_for(wc.at[pl.ds(lo, hi - lo)], c_rs.at[p])
        for k in range(lo, hi):
            for pz in range(2):
                @pl.loop(0, NX)
                def _(px):
                    v = (w32[k, c, pz, px] + wc[k, pz, px]).reshape(HC, 16, 128)
                    xs[pz, px, (k - lo) * HC:(k - lo + 1) * HC] = v.astype(BF16)
        for cp in x_cp[p]:
            cp.start()
    heard(1)
    tell(2)

    inv = 1.0 / (NY * pvg.shape[2])

    def d_conv(lo, hi, yr):
        for b in range(lo // 4, (hi + 3) // 4):
            rows = pl.ds(128 * b, 128)
            tot = ((yr[0, b] + yr[1, b]) + (yr[2, b] + yr[3, b])) * inv
            s1[rows, :] = jnp.broadcast_to(tot[0:1, :], (128, 128)).T
            s2[rows, :] = jnp.broadcast_to(tot[1:2, :], (128, 128)).T

        @pl.loop(lo, hi)
        def _(i):
            sl = pl.ds(pl.multiple_of(i * 32, 32), 32)
            for h in range(2):
                dcp[h, sl, :] = rs[sl, :] * (dn[h, sl, :] - s1[sl, :] - nm[h, sl, :] * s2[sl, :])

    def tap_rows(lo, hi, start):
        for h in range(2):
            def step(i, acc):
                acc = list(acc)
                for e in range(4):
                    r0 = pl.multiple_of(i * 32 + 8 * e, 8)
                    d = dcp[h, pl.ds(r0, 8), :]
                    for k in range(taps):
                        acc[k] = acc[k] + d * gp[h, pl.ds(r0 + (HALO + 1 - taps + k), 8), :]
                return tuple(acc)
            init = tuple(jnp.zeros((8, 128), F32) if start else kacc[h, k] for k in range(taps))
            acc = lax.fori_loop(lo, hi, step, init)
            for k in range(taps):
                if start:
                    kacc[h, k] = acc[k]
                else:
                    tp[k // 4, 4 * h + k % 4, :] = jnp.sum(acc[k], axis=0)
    wait_for(yr.at[pl.ds(0, NY - 1)], y_rs.at[0])
    d_conv(1, length // 32, yr)
    tap_rows(1, length // 32, True)
    for h in range(2):
        tp[taps // 4, 4 * h + taps % 4, :] = jnp.sum(gacc[h], axis=0)
    wait_for(yr0.at[pl.ds(0, NY - 1)], y_rs.at[1])
    d_conv(0, 1, yr0)
    dhalo = pltpu.make_async_remote_copy(
        dcp.at[:, pl.ds(0, HALO), :], dcp.at[:, pl.ds(length, HALO), :], dhalo_sem.at[0], dhalo_sem.at[1],
        device_id=prv, device_id_type=MESH)
    tap_rows(0, 1, False)
    t_cp = []
    for pz, px, q in owners:
        t_cp.append(pltpu.make_async_remote_copy(
            tp.at[pz * NX + px], tr.at[8 * c + g_me], t_ss, t_rs, device_id=mate(pz, px, 1), device_id_type=MESH))
    for cp in t_cp[:-1]:
        cp.start()

    @pl.when(c == 0)
    def _():
        t_cp[-1].start()

    @pl.when(c == 1)
    def _():
        tr[8 * c + g_me] = tp[g_me]
    dhalo.start()

    early = z < EARLY
    late = jnp.logical_not(early)
    x_phase(0)

    @pl.when(early)
    def _():
        x_phase(1)


    def d_gated(h, r0, rows):
        acc = jnp.zeros((rows, 128), F32)
        for k in range(taps):
            acc = acc + wt[h, k:k + 1, :] * dcp[h, pl.ds(r0 + (taps - 1 - k), rows), :]
        sl, lanes = pl.ds(r0, rows), pl.ds(128 * h, 128)
        s = sg[h, sl, :]
        vg_o[sl, lanes] = (acc * s).astype(BF16)
        gg_o[sl, lanes] = (acc * pvg[0, sl, lanes].astype(F32) * s * (1.0 - s)).astype(BF16)
    @pl.loop(0, 2 * ((length - HALO) // 32))
    def _(i):
        d_gated(rem(i, 2), pl.multiple_of(div(i, 2) * 32, 32), 32)

    def z_copy(src, dst, ss, rs_, d):
        return pltpu.make_async_remote_copy(
            src, dst, ss, rs_, device_id={"z": 2 * d + 1 - zp}, device_id_type=MESH)

    def tree(parts):
        while len(parts) > 1:
            parts = [a + b for a, b in zip(parts[::2], parts[1::2])] + parts[len(parts) // 2 * 2:]
        return parts[0]

    def z_phase(p):
        xs, xr, lo, hi = parts[p]
        wait_for(xr, x_rs.at[p])
        for k in range(lo, hi):
            v = (w32[k, c, 1 - zp, x] + wc[k, 1 - zp, x]).reshape(HC, 16, 128)
            for q in range(2 * NX - 1):
                v = v + xr[q, (k - lo) * HC:(k - lo + 1) * HC].astype(F32)
            zs[k * HC:(k + 1) * HC] = v.astype(BF16)
        for d in range(lo * HC, hi * HC):
            z_copy(zs.at[d], zr.at[zh], z_ss, z_rs, d).start()

    def share_out(lo, hi):
        for d in range(lo, hi):
            z_copy(tf.at[0], tz.at[zh], tz_ss, tz_rs, d).start()
    heard(2)


    @pl.when(c == 1)
    def _():
        wait_for(tr.at[pl.ds(0, 15)], t_rs)
        share = tree([tr[k] for k in range(16)])
        tf[0] = share
        share_out(0, FIRST)
    z_phase(0)
    @pl.when(early)
    def _():
        z_phase(1)

    @pl.when((c == 1) & early)
    def _():
        share_out(FIRST, NH)
    @pl.when(late)
    def _():
        x_phase(1)
    last_dev = ((z * NX + x) * NC + c) == NZ * NX * NC - 1
    dhalo.wait_recv()
    for h in range(2):
        got = dcp[h, pl.ds(length, HALO), :]
        dcp[h, pl.ds(length, HALO), :] = jnp.where(last_dev, jnp.zeros_like(got), got)
        d_gated(h, length - HALO, HALO)
    @pl.when(late)
    def _():
        z_phase(1)

    @pl.when((c == 1) & late)
    def _():
        share_out(FIRST, NH)

    halo.wait_send()
    dhalo.wait_send()
    wait_for(yr.at[pl.ds(0, NY - 1)], y_ss.at[0])
    wait_for(yr0.at[pl.ds(0, NY - 1)], y_ss.at[1])
    wait_for(wc, c_ss)
    for p in range(2):
        wait_for(parts[p][1], x_ss.at[p])

    @pl.when(c == 0)
    def _():
        wait_for(tp, t_ss)

    @pl.when(c == 1)
    def _():
        wait_for(tp.at[pl.ds(0, 7)], t_ss)

    def f_copy(to):
        return pltpu.make_async_remote_copy(
            tf.at[1], tacc.at[g_sum], tf_ss, tf_rs, device_id=mate(*to), device_id_type=MESH)

    @pl.when(c == 1)
    def _():
        wait_for(tz, tz_rs)
        total = tree([tz[i] for i in range(NH)])
        tf[1] = total
        for to in mates:
            f_copy(to).start()
        tacc[g_sum] = total

    wait_for(zr, z_rs)
    wsum = tree([zr[i].astype(F32) for i in range(NH)])
    for h in range(2):
        wg_o[:, pl.ds(128 * h, 128)] = wsum[8 * h:8 * h + 8, :]
    wait_for(zr, z_ss)

    @pl.when(c == 1)
    def _():
        wait_for(tz, tz_ss)

    @pl.when(c == 0)
    def _():
        wait_for(tacc, tf_rs)

    @pl.when(c == 1)
    def _():
        wait_for(tacc.at[pl.ds(0, 7)], tf_rs)
    for k in range(taps + 1):
        for h in range(2):
            row = tacc[k // 4, 4 * h + k % 4:4 * h + k % 4 + 1, :]
            if k < taps:
                tg_o[k:k + 1, pl.ds(128 * h, 128)] = row
            else:
                gn_o[pl.ds(128 * h, 128)] = row.reshape(128)

    @pl.when(c == 1)
    def _():
        wait_for(tr.at[pl.ds(0, 15)], tf_ss)


def out_kernel(*refs):
    n = len(refs) // 2
    sems = refs[-1]
    cps = [pltpu.make_async_copy(refs[k], refs[n + k], sems.at[k]) for k in range(n)]
    for cp in cps:
        cp.start()
    for cp in cps:
        cp.wait()


def shards(pv, pg, cot, ow, taps, gain, mean, scale):
    length, ch = pv.shape
    d = cot.shape[1]
    blocks = length // 128
    V, D = pltpu.VMEM, pltpu.SemaphoreType.DMA
    any_spec, vmem = pl.BlockSpec(memory_space=pl.ANY), pl.BlockSpec(memory_space=pltpu.VMEM)
    scratch = [
        V((2, length, ch), BF16), V((length, d), BF16), V((ch, d), BF16),
        V(taps.shape, BF16), V((ch,), F32), V((length,), F32), V((length,), F32),
        V((HALO, ch), BF16), V((HALO, ch), BF16),
        V((2, length + HALO, 128), F32), V((2, length, 128), F32), V((2, length, 128), F32),
        V((2, length, 128), F32), V((2, length, 128), F32), V((2, length, 128), F32),
        V((length, ch), BF16), V((2, length + HALO, 128), F32),
        V((length, 128), F32), V((length, 128), F32), V((length, 128), F32), V((length, 128), F32),
        V((2, 32, 128), F32), V((2, 8, 128), F32),
        V((d, length), BF16),
        V((blocks, 2, 128), F32), V((NY, blocks, 2, 128), F32), V((1, 2, 128), F32), V((NY, 1, 2, 128), F32),
        V((2, 32, 8, 128), F32),
        V((8, 8, 128), F32), V((8, 8, 128), F32), V((16, 8, 128), F32), V((NH, 8, 128), F32), V((2, 8, 128), F32),
        V((CHUNKS, NC, 2, NX, HC, 2, 8, 128), F32), V((CHUNKS, 2, NX, HC, 2, 8, 128), F32),
        V((2, NX, HC, 16, 128), BF16), V((2, NX, NH - HC, 16, 128), BF16),
        V((2 * NX - 1, HC, 16, 128), BF16), V((2 * NX - 1, NH - HC, 16, 128), BF16),
        V((NH, 16, 128), BF16), V((NH, 16, 128), BF16),
        D((7,)), D((2,)), D((2,)), D((2,)), D((2,)), D, D, D, D, D, D,
        D, D((2,)), D((2,)), D((2,)), D, D,
        pltpu.SemaphoreType.REGULAR((3,)),
    ]
    outs = (((length, ch), BF16), ((length, ch), BF16), ((8, ch), F32), (taps.shape, F32), ((ch,), F32))
    res = pl.pallas_call(
        main_kernel,
        out_shape=tuple(V(s, t) for s, t in outs),
        in_specs=[any_spec] * 8,
        out_specs=(vmem,) * 5,
        scratch_shapes=scratch,
        name="conv_back",
        compiler_params=pltpu.CompilerParams(collective_id=0, has_side_effects=True, vmem_limit_bytes=56 * 2**20),
    )(pv, pg, cot, ow, taps, gain, mean, scale)
    return pl.pallas_call(
        out_kernel,
        out_shape=tuple(jax.ShapeDtypeStruct(s, t) for s, t in outs),
        in_specs=[vmem] * 5,
        out_specs=(any_spec,) * 5,
        scratch_shapes=[D((5,))],
        name="write_out",
    )(*(pltpu.with_memory_space_constraint(r, pltpu.VMEM) for r in res))


def solution(mesh):
    split = Mesh(mesh.devices.reshape(NZ, NX, NC, mesh.shape["tp"]), ("z", "x", "c", "y"))
    placed = (P(SP, "y"), P(SP, "y"), P(SP, None), P("y", None), P(None, "y"), P("y"), P(SP), P(SP))
    return jax.shard_map(
        shards, mesh=split, in_specs=placed,
        out_specs=(P(SP, "y"), P(SP, "y"), P(SP, "y"), P(None, "y"), P("y")), check_vma=False,
    )
```
